512 devices in a mesh: sp: 64 (over z, y), tp: 8 (over x, core).
Axes of the slice: x: 4, y: 8, z: 8, core: 2. Of those that a mesh axis runs over, the one named last changes fastest.
Arguments:
- inputs: bfloat16 [24576, 2048], P(('sp', 'tp')), may hold values from -6 to 6
- norm_gain: float32 [2048], replicated, may hold values from 0.1 to 1.9
- latent_down: bfloat16 [2048, 256], P('sp'), may hold values from -0.125 to 0.125
- rope_down: bfloat16 [2048, 64], P('sp'), may hold values from -0.125 to 0.125
- latent_gain: float32 [256], replicated, may hold values from 0.1 to 1.9
- mla_query: bfloat16 [2048, 1536], P(None, 'tp'), as said below
- key_up: bfloat16 [256, 1024], replicated, may hold values from -3.5 to 3.5
- value_up: bfloat16 [256, 1024], replicated, may hold values from -1.75 to 1.75
- swa_query: bfloat16 [2048, 1024], P(None, 'tp'), as said below
- swa_key: bfloat16 [2048, 512], P(None, 'tp'), may hold values from -0.125 to 0.125
- swa_value: bfloat16 [2048, 512], P(None, 'tp'), may hold values from -0.125 to 0.125
- sink_logits: float32 [16], replicated, may hold values from 1 to 6
- out_mla: bfloat16 [1024, 2048], P(None, 'tp'), may hold values from -0.875 to 0.875
- out_swa: bfloat16 [1024, 2048], P(None, 'tp'), may hold values from -0.875 to 0.875
Outputs:
- mixed: bfloat16 [24576, 2048], P('sp', 'tp')
The draws below stay inside these ranges and needn't reach their ends.
Inputs may be any that keep to these rules, and one draw needn't show every extreme that they name: `mla_query`: entries lie within 360 / sqrt(2048) in magnitude. `swa_query`: entries lie within 900 / sqrt(2048) in magnitude.
All inputs are finite; a program needn't handle non-finite values.
Results may differ from the reference program's by a relative error of at most 0.02.
The reference program's roundings to bfloat16 on the way count: a program that leaves them out, or rounds other values in their place, can miss the bound.
Values may be sent and summed in bfloat16 or wider, within the bound.
No kernel may reach another device: no remote copies, remote signals or barrier semaphores. Data moves between devices by JAX's collectives and lax.ppermute only.
A program may use at most 64 MiB of HBM per device.

```python
import math
import jax
import jax.numpy as jnp
from jax import lax

D = 2048
MLA_HEADS = 8
NOPE = 128
ROPE = 64
VDIM = 128
KV_RANK = 256
SWA_HEADS = 16
SWA_KV = 8
HEAD = 64
WINDOW = 128
SEQ = 24576


def draw_mla_query(key, part):
    values = jnp.clip(jax.random.normal(key, (D, MLA_HEADS * (NOPE + ROPE)), jnp.float32), -6.0, 6.0)
    values = values * D ** (-0.5)
    return values.astype(jnp.bfloat16)


def draw_swa_query(key, part):
    values = jnp.clip(jax.random.normal(key, (D, SWA_HEADS * HEAD), jnp.float32), -6.0, 6.0)
    values = values * (1.5 * D ** (-0.5))
    return values.astype(jnp.bfloat16)


def block_scale(rng, shape, shards, low, high):
    level = 1.0
    for position, blocks in shards:
        steps = jax.random.uniform(jax.random.fold_in(jax.random.fold_in(rng, 6), position), (blocks,), jnp.float32, low / len(shards), high / len(shards))
        level = level * jnp.repeat(jnp.exp(steps), shape[position] // blocks).reshape((-1,) + (1,) * (len(shape) - 1 - position))
    return level


def noise(rng, dims, deviation, bound, pieces=(), kind=jnp.bfloat16):
    array = deviation * jax.random.normal(rng, dims, jnp.float32)
    if pieces:
        array = array * block_scale(rng, dims, pieces, -0.22, 0.18)
    return jnp.clip(array, -bound, bound).astype(kind)


def setup_inputs(seed: int = 0) -> dict:
    key_list = jax.random.split(jax.random.key(seed), 15)
    inputs = noise(key_list[0], (SEQ, D), 1.0, 6.0, ((0, 512),))
    norm_gain = jnp.clip(1.0 + 0.18 * jax.random.normal(key_list[1], (D,), jnp.float32), 0.1, 1.9)
    latent_down = noise(key_list[2], (D, KV_RANK), D ** -0.5, 0.125, ((0, 64),))
    rope_down = noise(key_list[3], (D, ROPE), D ** -0.5, 0.125, ((0, 64),))
    latent_gain = jnp.clip(1.0 + 0.18 * jax.random.normal(key_list[4], (KV_RANK,), jnp.float32), 0.1, 1.9)
    mla_query = draw_mla_query(jax.random.fold_in(key_list[14], 71), 0)
    key_up = noise(key_list[6], (KV_RANK, MLA_HEADS * NOPE), 0.22, 3.5)
    value_up = noise(key_list[7], (KV_RANK, MLA_HEADS * VDIM), 0.12, 1.75)
    swa_query = draw_swa_query(jax.random.fold_in(key_list[14], 71), 0)
    swa_key = noise(key_list[9], (D, SWA_KV * HEAD), D ** -0.5, 0.125, ((1, 8),))
    swa_value = noise(key_list[10], (D, SWA_KV * HEAD), D ** -0.5, 0.125, ((1, 8),))
    sink_logits = jnp.clip(jax.random.uniform(key_list[11], (SWA_HEADS,), jnp.float32, 1.0, 6.0), 1.0, 6.0)
    out_mla = noise(key_list[12], (MLA_HEADS * VDIM, D), 0.06, 0.875, ((1, 8),))
    out_swa = noise(key_list[13], (SWA_HEADS * HEAD, D), 0.06, 0.875, ((1, 8),))
    return dict(inputs=inputs, norm_gain=norm_gain, latent_down=latent_down, rope_down=rope_down, latent_gain=latent_gain, mla_query=mla_query, key_up=key_up, value_up=value_up, swa_query=swa_query, swa_key=swa_key, swa_value=swa_value, sink_logits=sink_logits, out_mla=out_mla, out_swa=out_swa)


NORM_EPS = 1e-06
ROPE_BASE = 10000.0
MASKED_VALUE = -1e+30

def to_float(values):
    return lax.optimization_barrier(values).astype(jnp.float32)

def norm_rows(values, gains):
    widened = to_float(values)
    scaled = widened * lax.rsqrt(lax.optimization_barrier(jnp.mean(widened * widened, axis=-1, keepdims=True)) + NORM_EPS)
    return (scaled * gains).astype(jnp.bfloat16)

def rotate(values, positions):
    full_width = values.shape[-1]
    half_width = full_width // 2
    inverse = ROPE_BASE ** (-jnp.arange(0, full_width, 2, dtype=jnp.float32) / full_width)
    angles = positions.astype(jnp.float32)[:, None] * inverse[None, :]
    shaped = (values.shape[0],) + (1,) * (values.ndim - 2) + (half_width,)
    cos_table = jnp.cos(angles).reshape(shaped)
    sin_table = jnp.sin(angles).reshape(shaped)
    widened = to_float(values)
    first_half = widened[..., :half_width]
    second_half = widened[..., half_width:]
    return jnp.concatenate([first_half * cos_table - second_half * sin_table, first_half * sin_table + second_half * cos_table], axis=-1).astype(jnp.bfloat16)

def reference(inputs, norm_gain, latent_down, rope_down, latent_gain, mla_query, key_up, value_up, swa_query, swa_key, swa_value, sink_logits, out_mla, out_swa):
    length = inputs.shape[0]
    positions = jnp.arange(length, dtype=jnp.int32)
    normed = norm_rows(inputs, norm_gain)
    latent = jnp.dot(normed, latent_down, preferred_element_type=jnp.float32).astype(jnp.bfloat16)
    keys_latent = norm_rows(latent, latent_gain)
    rope_raw = jnp.dot(normed, rope_down, preferred_element_type=jnp.float32).astype(jnp.bfloat16)
    keys_rope = rotate(rope_raw, positions)
    queries = jnp.dot(normed, mla_query, preferred_element_type=jnp.float32).astype(jnp.bfloat16)
    queries = queries.reshape(length, MLA_HEADS, NOPE + ROPE)
    query_rope = jnp.transpose(rotate(queries[:, :, NOPE:], positions), (1, 0, 2))
    up_keys = key_up.reshape(KV_RANK, MLA_HEADS, NOPE)
    query_latent = jnp.einsum('thn,jhn->htj', to_float(queries[:, :, :NOPE]), to_float(up_keys)).astype(jnp.bfloat16)
    span_rows = math.gcd(length, 512)
    span_count = length // span_rows
    mla_scale = (NOPE + ROPE) ** (-0.5)
    keys_wide = to_float(keys_latent)
    rope_wide = to_float(keys_rope)

    def mla_span(span_index):
        anchor = span_index * span_rows
        lat_block = lax.dynamic_slice_in_dim(query_latent, anchor, span_rows, 1)
        rope_block = lax.dynamic_slice_in_dim(query_rope, anchor, span_rows, 1)
        scores = (jnp.einsum('htj,sj->hts', to_float(lat_block), keys_wide) + jnp.einsum('htd,sd->hts', to_float(rope_block), rope_wide)) * mla_scale
        query_pos = anchor + jnp.arange(span_rows, dtype=jnp.int32)
        allowed = positions[None, None, :] <= query_pos[None, :, None]
        scores = jnp.where(allowed, scores, MASKED_VALUE)
        row_max = lax.optimization_barrier(jnp.max(scores, axis=-1, keepdims=True))
        weights_raw = jnp.where(allowed, jnp.exp(scores - row_max), 0.0)
        denom_sum = lax.optimization_barrier(jnp.sum(weights_raw, axis=-1, keepdims=True))
        weighted = jnp.einsum('hts,sj->htj', to_float(weights_raw.astype(jnp.bfloat16)), keys_wide)
        return (weighted / denom_sum).astype(jnp.bfloat16)
    latent_out = lax.map(mla_span, jnp.arange(span_count, dtype=jnp.int32))
    latent_out = jnp.transpose(latent_out, (1, 0, 2, 3)).reshape(MLA_HEADS, length, KV_RANK)
    up_values = value_up.reshape(KV_RANK, MLA_HEADS, VDIM)
    mla_out = jnp.einsum('htj,jhv->thv', to_float(latent_out), to_float(up_values)).astype(jnp.bfloat16)
    mla_out = mla_out.reshape(length, MLA_HEADS * VDIM)
    group = SWA_HEADS // SWA_KV
    swa_q = jnp.dot(normed, swa_query, preferred_element_type=jnp.float32).astype(jnp.bfloat16)
    swa_q = swa_q.reshape(length, SWA_KV, group, HEAD)
    swa_k = jnp.dot(normed, swa_key, preferred_element_type=jnp.float32).astype(jnp.bfloat16)
    swa_k = swa_k.reshape(length, SWA_KV, HEAD)
    swa_v = jnp.dot(normed, swa_value, preferred_element_type=jnp.float32).astype(jnp.bfloat16)
    swa_v = swa_v.reshape(length, SWA_KV, HEAD)
    padding = jnp.zeros((WINDOW, SWA_KV, HEAD), jnp.bfloat16)
    keys_pad = jnp.concatenate([padding, swa_k], axis=0)
    values_pad = jnp.concatenate([padding, swa_v], axis=0)
    sink_table = sink_logits.reshape(SWA_KV, group, 1, 1)

    def swa_span(span_index):
        anchor = span_index * span_rows
        query_block = lax.dynamic_slice_in_dim(swa_q, anchor, span_rows, 0)
        key_block = lax.dynamic_slice_in_dim(keys_pad, anchor, span_rows + WINDOW, 0)
        value_block = lax.dynamic_slice_in_dim(values_pad, anchor, span_rows + WINDOW, 0)
        scores = jnp.einsum('tkgd,skd->kgts', to_float(query_block), to_float(key_block)) * HEAD ** (-0.5)
        query_pos = anchor + jnp.arange(span_rows, dtype=jnp.int32)
        key_pos = anchor - WINDOW + jnp.arange(span_rows + WINDOW, dtype=jnp.int32)
        distance = query_pos[:, None] - key_pos[None, :]
        allowed = (distance >= 0) & (distance < WINDOW) & (key_pos[None, :] >= 0)
        scores = jnp.where(allowed, scores, MASKED_VALUE)
        row_max = jnp.maximum(lax.optimization_barrier(jnp.max(scores, axis=-1, keepdims=True)), sink_table)
        weights_raw = jnp.exp(scores - row_max)
        weights = (weights_raw / (lax.optimization_barrier(jnp.sum(weights_raw, axis=-1, keepdims=True)) + jnp.exp(sink_table - row_max))).astype(jnp.bfloat16)
        return jnp.einsum('kgts,skd->tkgd', to_float(weights), to_float(value_block)).astype(jnp.bfloat16)
    swa_out = lax.map(swa_span, jnp.arange(span_count, dtype=jnp.int32)).reshape(length, SWA_HEADS * HEAD)
    mixed = jnp.dot(mla_out, out_mla, preferred_element_type=jnp.float32) + jnp.dot(swa_out, out_swa, preferred_element_type=jnp.float32)
    return mixed.astype(jnp.bfloat16)
```

```python
import functools
import math

import jax
import jax.numpy as jnp
from jax import lax
from jax.experimental import pallas as pl
from jax.experimental.pallas import tpu as pltpu
from jax.sharding import Mesh
from jax.sharding import PartitionSpec as P

NOPE = 128
ROPE = 64
VDIM = 128
KV_RANK = 256
HEAD = 64
WINDOW = 128
SP = ("z", "y")
TP = ("x", "c")
SP_TP = ("z", "y", "x", "c")

NORM_EPS = 1e-06
ROPE_BASE = 10000.0
MASKED_VALUE = -1e30
LANES = 128
OWN = 48
SOURCES = 64
ROWS = 384
CHUNK = 16
QTILE = 256
HEADS_CORE = 4
QROWS = HEADS_CORE * ROWS
TILES = QROWS // QTILE
STAT_ROWS = 16
EXP_SCALE = (NOPE + ROPE) ** (-0.5) * math.log2(math.e)


def exchange(array, axis):
    return lax.all_to_all(array, axis, split_axis=0, concat_axis=0, tiled=True)


def to_everyone(array, axis):
    copies = jnp.broadcast_to(array, (lax.axis_size(axis), *array.shape))
    return exchange(copies, axis)


def from_core(value):
    return lax.ppermute(value, "c", [(0, 1), (1, 0)])


def from_x(value, step):
    count = lax.axis_size("x")
    return lax.ppermute(value, "x", [(i, (i + step) % count) for i in range(count)])


def to_float(values):
    return lax.optimization_barrier(values).astype(jnp.float32)


def norm_rows(values, gains):
    widened = to_float(values)
    scaled = widened * lax.rsqrt(jnp.mean(widened * widened, axis=-1, keepdims=True) + NORM_EPS)
    return (scaled * gains).astype(jnp.bfloat16)


def rotate(values, positions):
    full_width = values.shape[-1]
    half_width = full_width // 2
    inverse = ROPE_BASE ** (-jnp.arange(0, full_width, 2, dtype=jnp.float32) / full_width)
    angles = positions.astype(jnp.float32)[:, None] * inverse[None, :]
    cos_table = jnp.cos(angles)
    sin_table = jnp.sin(angles)
    widened = to_float(values)
    first_half = widened[..., :half_width]
    second_half = widened[..., half_width:]
    return jnp.concatenate(
        [
            first_half * cos_table - second_half * sin_table,
            first_half * sin_table + second_half * cos_table,
        ],
        axis=-1,
    ).astype(jnp.bfloat16)


def attend_body(where_ref, keys_ref, q_ref, *refs, first, last):
    if first:
        (o_ref, m_ref, l_ref, kc_ref, vt_ref) = refs
    elif last:
        (o_in, m_in, l_in, out_ref, o_ref, m_ref, l_ref, kc_ref, vt_ref) = refs
    block = where_ref[0]
    key_rank = where_ref[1]
    if first:
        o_ref[...] = jnp.zeros_like(o_ref)
        m_ref[...] = jnp.full(m_ref.shape, MASKED_VALUE, jnp.float32)
        l_ref[...] = jnp.zeros_like(l_ref)
    else:
        o_ref[...] = o_in[...]
        m_ref[...] = m_in[...]
        l_ref[...] = l_in[...]
    n_keys = CHUNK * OWN

    def chunk_step(index, masked):
        part = keys_ref[pl.ds(index * CHUNK, CHUNK)]
        k0 = part[:, :OWN].reshape(n_keys, LANES)
        k1 = part[:, OWN : 2 * OWN].reshape(n_keys, LANES)
        t0 = part[:, 2 * OWN : 2 * OWN + 16]
        t1 = part[:, 2 * OWN + 16 :]
        t0s = jnp.concatenate([t0[..., ROPE:], t0[..., :ROPE]], axis=-1)
        kr = jnp.stack([t0, t0s, t1], axis=1).reshape(n_keys, LANES)
        kc_ref[:, :LANES] = k0
        kc_ref[:, LANES : 2 * LANES] = k1
        kc_ref[:, 2 * LANES :] = kr
        vt_ref[:LANES] = k0.T
        vt_ref[LANES:] = k1.T
        if masked:
            row = lax.broadcasted_iota(jnp.int32, (n_keys, 1), 0)
            key_pos = (index * CHUNK + row // OWN) * ROWS + key_rank * OWN + row % OWN

        def tile_step(tile):
            q = q_ref[pl.ds(tile * QTILE, QTILE)]
            s = lax.dot_general(
                kc_ref[...], q, (((1,), (1,)), ((), ())), preferred_element_type=jnp.float32
            )
            if masked:
                col = tile * QTILE + lax.broadcasted_iota(jnp.int32, (1, QTILE), 1)
                allowed = key_pos <= block * ROWS + col % ROWS
                s = jnp.where(allowed, s, MASKED_VALUE)
            old = m_ref[tile]
            new = jnp.maximum(old, jnp.max(s, axis=0, keepdims=True))
            p = jnp.exp2((s - new) * EXP_SCALE)
            if masked:
                p = jnp.where(allowed, p, 0.0)
            alpha = jnp.exp2((old - new) * EXP_SCALE)
            m_ref[tile] = new
            l_ref[tile] = l_ref[tile] * alpha + jnp.sum(p, axis=0, keepdims=True)
            o_ref[tile] = o_ref[tile] * alpha + jnp.dot(
                vt_ref[...], p.astype(jnp.bfloat16), preferred_element_type=jnp.float32
            )

        def pair_step(pair, carry):
            tile_step(2 * pair)
            tile_step(2 * pair + 1)
            return carry

        lax.fori_loop(0, TILES // 2, pair_step, 0)

    def full_step(index, carry):
        chunk_step(index, False)
        return carry

    n_full = block // CHUNK
    lax.fori_loop(0, n_full, full_step, 0)
    chunk_step(n_full, True)
    if last:
        whole = jnp.concatenate([o_ref[t] for t in range(TILES)], axis=1).astype(jnp.bfloat16)
        m = jnp.concatenate([m_ref[t] for t in range(TILES)], axis=1)
        l = jnp.concatenate([l_ref[t] for t in range(TILES)], axis=1)
        m0 = m.astype(jnp.bfloat16).astype(jnp.float32)
        m1 = (m - m0).astype(jnp.bfloat16).astype(jnp.float32)
        m2 = m - m0 - m1
        l0 = l.astype(jnp.bfloat16).astype(jnp.float32)
        l1 = l - l0
        pad = jnp.zeros((STAT_ROWS - 5, QROWS), jnp.float32)
        stats = jnp.concatenate([m0, m1, m2, l0, l1, pad], axis=0).astype(jnp.bfloat16)
        for h in range(HEADS_CORE):
            out_ref[h, :KV_RANK] = whole[:, h * ROWS : (h + 1) * ROWS]
            out_ref[h, KV_RANK:] = stats[:, h * ROWS : (h + 1) * ROWS]


def attend(where, keys, q, state):
    state_shapes = (
        jax.ShapeDtypeStruct((TILES, KV_RANK, QTILE), jnp.float32),
        jax.ShapeDtypeStruct((TILES, 1, QTILE), jnp.float32),
        jax.ShapeDtypeStruct((TILES, 1, QTILE), jnp.float32),
    )
    first = state is None
    smem = pl.BlockSpec(memory_space=pltpu.SMEM)
    vmem = pl.BlockSpec(memory_space=pltpu.VMEM)
    scratch = [
        pltpu.VMEM((CHUNK * OWN, 3 * LANES), jnp.bfloat16),
        pltpu.VMEM((KV_RANK, CHUNK * OWN), jnp.bfloat16),
    ]
    if not first:
        scratch = [pltpu.VMEM(s.shape, s.dtype) for s in state_shapes] + scratch
    out_shape = (
        state_shapes
        if first
        else jax.ShapeDtypeStruct((HEADS_CORE, KV_RANK + STAT_ROWS, ROWS), jnp.bfloat16)
    )
    operands = (where, keys, q) + (() if first else tuple(state))
    flops = 2 * QROWS * SOURCES * OWN * (3 * LANES + KV_RANK)
    return pl.pallas_call(
        functools.partial(attend_body, first=first, last=not first),
        out_shape=out_shape,
        in_specs=[smem] + [vmem] * (len(operands) - 1),
        out_specs=jax.tree.map(lambda _: vmem, out_shape),
        scratch_shapes=scratch,
        cost_estimate=pl.CostEstimate(
            flops=flops, transcendentals=QROWS * SOURCES * OWN, bytes_accessed=6000000
        ),
        name="attend_first" if first else "attend_last",
    )(*operands)


def shards(
    inputs,
    norm_gain,
    latent_down,
    rope_down,
    latent_gain,
    mla_query,
    key_up,
    value_up,
    swa_query,
    swa_key,
    swa_value,
    sink_logits,
    out_mla,
    out_swa,
):
    own_rows = inputs.shape[0]
    x_rank = lax.axis_index("x")
    c_rank = lax.axis_index("c")
    tp_rank = lax.axis_index(TP)
    block = lax.axis_index(SP)
    offset = block * ROWS
    own_pos = offset + tp_rank * own_rows + jnp.arange(own_rows, dtype=jnp.int32)
    block_pos = offset + jnp.arange(ROWS, dtype=jnp.int32)
    heads_swa = swa_query.shape[1] // HEAD

    down = jnp.concatenate([latent_down, rope_down], axis=1)
    width = down.shape[1] // lax.axis_size(TP)
    down = lax.dynamic_slice_in_dim(down, tp_rank * width, width, 1)
    half = down.shape[0] // 2
    fill = ((0, 0), (0, LANES // 2 - width))
    down = jnp.concatenate([jnp.pad(down[:half], fill), jnp.pad(down[half:], fill)], axis=1)
    down = to_everyone(down, SP)
    down = jnp.stack([down[:, :, :width], down[:, :, LANES // 2 : LANES // 2 + width]], axis=1)
    down = down.reshape(-1, width)

    normed = norm_rows(inputs, norm_gain)
    mine = to_everyone(normed, "x")
    other = from_core(mine)
    is_first = c_rank == 0
    pieces = jnp.stack([jnp.where(is_first, mine, other), jnp.where(is_first, other, mine)], axis=1)
    pieces = pieces.reshape(ROWS, -1)

    latent = jnp.dot(pieces, down, preferred_element_type=jnp.float32).astype(jnp.bfloat16)
    latent = exchange(latent.reshape(-1, own_rows, width), TP)
    latent = jnp.transpose(latent, (1, 0, 2)).reshape(own_rows, KV_RANK + ROPE)
    keys_latent = norm_rows(latent[:, :KV_RANK], latent_gain)
    keys_rope = rotate(latent[:, KV_RANK:], own_pos)
    packed = jnp.concatenate(
        [
            keys_latent[:, :LANES],
            keys_latent[:, LANES:],
            jnp.concatenate([keys_rope[:16], keys_rope[16:32]], axis=1),
            jnp.concatenate([keys_rope[32:], jnp.zeros((16, ROPE), jnp.bfloat16)], axis=1),
        ],
        axis=0,
    )
    packed, pieces = lax.optimization_barrier((packed, pieces))
    keys_own = to_everyone(packed, SP)

    queries = jnp.dot(pieces, mla_query, preferred_element_type=jnp.float32).astype(jnp.bfloat16)
    swa_q = jnp.dot(pieces, swa_query, preferred_element_type=jnp.float32).astype(jnp.bfloat16)
    swa_k = jnp.dot(pieces, swa_key, preferred_element_type=jnp.float32).astype(jnp.bfloat16)
    swa_v = jnp.dot(pieces, swa_value, preferred_element_type=jnp.float32).astype(jnp.bfloat16)
    query = jnp.concatenate(
        [
            queries[:, :NOPE],
            rotate(queries[:, NOPE:], block_pos),
            jnp.zeros((ROWS, LANES - ROPE), jnp.bfloat16),
        ],
        axis=1,
    )
    around = jnp.stack([query] + [from_x(query, k) for k in range(1, 4)], axis=0)
    q_heads = []
    for j in range(HEADS_CORE):
        q_j = lax.dynamic_index_in_dim(around, (x_rank - j) % HEADS_CORE, 0, keepdims=False)
        up = lax.dynamic_slice_in_dim(key_up, (2 * j + c_rank) * NOPE, NOPE, 1)
        lat = lax.dot_general(
            q_j[:, :NOPE], up, (((1,), (1,)), ((), ())), preferred_element_type=jnp.float32
        ).astype(jnp.bfloat16)
        q_heads.append(jnp.concatenate([lat, q_j[:, NOPE:]], axis=1))
    q_all = jnp.concatenate(q_heads, axis=0)

    tail = jnp.concatenate([swa_k[ROWS - WINDOW :], swa_v[ROWS - WINDOW :]], axis=1)
    count = lax.axis_size(SP)
    before = lax.ppermute(tail, SP, [(i, i + 1) for i in range(count - 1)])
    window_keys = jnp.concatenate([before[:, :HEAD], swa_k], axis=0)
    window_values = jnp.concatenate([before[:, HEAD:], swa_v], axis=0)
    scores = jnp.einsum(
        "tgd,sd->gts",
        swa_q.reshape(ROWS, heads_swa, HEAD),
        window_keys,
        preferred_element_type=jnp.float32,
    ) * HEAD ** (-0.5)
    key_pos = offset - WINDOW + jnp.arange(WINDOW + ROWS, dtype=jnp.int32)
    distance = block_pos[:, None] - key_pos[None, :]
    allowed = (distance >= 0) & (distance < WINDOW) & (key_pos[None, :] >= 0)
    scores = jnp.where(allowed, scores, MASKED_VALUE)
    sink = lax.dynamic_slice_in_dim(sink_logits, tp_rank * heads_swa, heads_swa, 0)
    sink = sink.reshape(heads_swa, 1, 1)
    row_max = jnp.maximum(jnp.max(scores, axis=-1, keepdims=True), sink)
    raw = jnp.exp(scores - row_max)
    weights = (
        raw / (jnp.sum(raw, axis=-1, keepdims=True) + jnp.exp(sink - row_max))
    ).astype(jnp.bfloat16)
    swa_out = jnp.einsum("gts,sd->tgd", weights, window_values, preferred_element_type=jnp.float32)
    swa_out = swa_out.astype(jnp.bfloat16).reshape(ROWS, heads_swa * HEAD)

    swa_out, keys_own = lax.optimization_barrier((swa_out, keys_own))
    keys_other = from_core(keys_own)
    rank_own = jnp.stack([block, tp_rank]).astype(jnp.int32)
    rank_other = jnp.stack([block, tp_rank + 1 - 2 * c_rank]).astype(jnp.int32)
    state = attend(rank_own, keys_own, q_all, None)
    partial = attend(rank_other, keys_other, q_all, state)
    all_swa = to_everyone(swa_out, TP)
    parts = exchange(partial, "x").astype(jnp.float32)
    stats = parts[:, KV_RANK:]
    m = stats[:, 0] + stats[:, 1] + stats[:, 2]
    l = stats[:, 3] + stats[:, 4]
    w = jnp.exp2((m - jnp.max(m, axis=0)) * EXP_SCALE)
    denominator = jnp.sum(l * w, axis=0)
    weighted = jnp.sum(parts[:, :KV_RANK] * w[:, None], axis=0)
    latent_out = (weighted / denominator).astype(jnp.bfloat16)
    up = lax.dynamic_slice_in_dim(value_up, tp_rank * VDIM, VDIM, 1)
    mla_out = lax.dot_general(
        latent_out, up, (((0,), (0,)), ((), ())), preferred_element_type=jnp.float32
    ).astype(jnp.bfloat16)
    all_mla = to_everyone(mla_out, TP)
    from_swa = jnp.einsum(
        "rtd,rdn->tn", all_swa, out_swa.reshape(8, -1, 256), preferred_element_type=jnp.float32
    )
    from_mla = jnp.einsum(
        "rtd,rdn->tn", all_mla, out_mla.reshape(8, -1, 256), preferred_element_type=jnp.float32
    )
    return (from_mla + from_swa).astype(jnp.bfloat16)


def solution(mesh):
    split = Mesh(mesh.devices.reshape(8, 8, 4, 2), SP_TP)
    placed = (
        P(SP_TP, None),
        P(),
        P(SP, None),
        P(SP, None),
        P(),
        P(None, TP),
        P(),
        P(),
        P(None, TP),
        P(None, TP),
        P(None, TP),
        P(),
        P(None, TP),
        P(None, TP),
    )
    return jax.shard_map(
        shards, mesh=split, in_specs=placed, out_specs=P(SP, TP), check_vma=False
    )
```

```python
import functools
import math

import jax
import jax.numpy as jnp
from jax import lax
from jax.experimental import pallas as pl
from jax.experimental.pallas import tpu as pltpu
from jax.sharding import Mesh
from jax.sharding import PartitionSpec as P


NOPE = 128
ROPE = 64
VDIM = 128
KV_RANK = 256
HEAD = 64
WINDOW = 128
SP = ("z", "y")
TP = ("x", "c")
SP_TP = ("z", "y", "x", "c")

NORM_EPS = 1e-06
ROPE_BASE = 10000.0
MASKED_VALUE = -1e30
LANES = 128
OWN = 48
SOURCES = 64
ROWS = 384
CHUNK = 16
QTILE = 512
HEADS_CORE = 4
QROWS = HEADS_CORE * ROWS
TILES = QROWS // QTILE
STAT_ROWS = 16
EXP_SCALE = (NOPE + ROPE) ** (-0.5) * math.log2(math.e)


def exchange(array, axis):
    return lax.all_to_all(array, axis, split_axis=0, concat_axis=0, tiled=True)


def to_everyone(array, axis):
    copies = jnp.broadcast_to(array, (lax.axis_size(axis), *array.shape))
    return exchange(copies, axis)


def from_core(value):
    return lax.ppermute(value, "c", [(0, 1), (1, 0)])


def from_x(value, step):
    count = lax.axis_size("x")
    return lax.ppermute(value, "x", [(i, (i + step) % count) for i in range(count)])


def to_float(values):
    return lax.optimization_barrier(values).astype(jnp.float32)


def norm_rows(values, gains):
    widened = to_float(values)
    scaled = widened * lax.rsqrt(jnp.mean(widened * widened, axis=-1, keepdims=True) + NORM_EPS)
    return (scaled * gains).astype(jnp.bfloat16)


def rotate(values, positions):
    full_width = values.shape[-1]
    half_width = full_width // 2
    inverse = ROPE_BASE ** (-jnp.arange(0, full_width, 2, dtype=jnp.float32) / full_width)
    angles = positions.astype(jnp.float32)[:, None] * inverse[None, :]
    cos_table = jnp.cos(angles)
    sin_table = jnp.sin(angles)
    widened = to_float(values)
    first_half = widened[..., :half_width]
    second_half = widened[..., half_width:]
    return jnp.concatenate(
        [
            first_half * cos_table - second_half * sin_table,
            first_half * sin_table + second_half * cos_table,
        ],
        axis=-1,
    ).astype(jnp.bfloat16)


def attend_body(where_ref, keys_ref, q_ref, *refs, first, last):
    if first:
        (o_ref, m_ref, l_ref, kc_ref, vt_ref) = refs
    elif last:
        (o_in, m_in, l_in, out_ref, o_ref, m_ref, l_ref, kc_ref, vt_ref) = refs
    block = where_ref[0]
    key_rank = where_ref[1]
    if first:
        o_ref[...] = jnp.zeros_like(o_ref)
        m_ref[...] = jnp.full(m_ref.shape, MASKED_VALUE, jnp.float32)
        l_ref[...] = jnp.zeros_like(l_ref)
    else:
        o_ref[...] = o_in[...]
        m_ref[...] = m_in[...]
        l_ref[...] = l_in[...]
    n_keys = CHUNK * OWN

    def chunk_step(index, masked):
        part = keys_ref[pl.ds(index * CHUNK, CHUNK)]
        k0 = part[:, :OWN].reshape(n_keys, LANES)
        k1 = part[:, OWN : 2 * OWN].reshape(n_keys, LANES)
        t0 = part[:, 2 * OWN : 2 * OWN + 16]
        t1 = part[:, 2 * OWN + 16 :]
        t0s = jnp.concatenate([t0[..., ROPE:], t0[..., :ROPE]], axis=-1)
        kr = jnp.stack([t0, t0s, t1], axis=1).reshape(n_keys, LANES)
        kc_ref[:, :LANES] = k0
        kc_ref[:, LANES : 2 * LANES] = k1
        kc_ref[:, 2 * LANES :] = kr
        if masked:
            row = lax.broadcasted_iota(jnp.int32, (n_keys, 1), 0)
            key_pos = (index * CHUNK + row // OWN) * ROWS + key_rank * OWN + row % OWN

        def scores_of(tile):
            return lax.dot_general(
                kc_ref[...],
                q_ref[tile * QTILE : (tile + 1) * QTILE],
                (((1,), (1,)), ((), ())),
                preferred_element_type=jnp.float32,
            )

        def absorb(tile, s):
            if masked:
                col = tile * QTILE + lax.broadcasted_iota(jnp.int32, (1, QTILE), 1)
                allowed = key_pos <= block * ROWS + col % ROWS
                s = jnp.where(allowed, s, MASKED_VALUE)
            old = m_ref[tile]
            new = jnp.maximum(old, jnp.max(s, axis=0, keepdims=True))
            p = jnp.exp2((s - new) * EXP_SCALE)
            if masked:
                p = jnp.where(allowed, p, 0.0)
            alpha = jnp.exp2((old - new) * EXP_SCALE)
            m_ref[tile] = new
            l_ref[tile] = l_ref[tile] * alpha + jnp.sum(p, axis=0, keepdims=True)
            o_ref[tile] = o_ref[tile] * alpha + lax.dot_general(
                kc_ref[:, : 2 * LANES], p.astype(jnp.bfloat16), (((0,), (0,)), ((), ())), preferred_element_type=jnp.float32
            )

        s = scores_of(0)
        for tile in range(TILES):
            ahead = scores_of(tile + 1) if tile + 1 < TILES else None
            absorb(tile, s)
            s = ahead

    def full_step(index, carry):
        chunk_step(index, False)
        return carry

    n_full = block // CHUNK
    lax.fori_loop(0, n_full, full_step, 0)
    chunk_step(n_full, True)
    if last:
        whole = jnp.concatenate([o_ref[t] for t in range(TILES)], axis=1).astype(jnp.bfloat16)
        m = jnp.concatenate([m_ref[t] for t in range(TILES)], axis=1)
        l = jnp.concatenate([l_ref[t] for t in range(TILES)], axis=1)
        m0 = m.astype(jnp.bfloat16).astype(jnp.float32)
        m1 = (m - m0).astype(jnp.bfloat16).astype(jnp.float32)
        m2 = m - m0 - m1
        l0 = l.astype(jnp.bfloat16).astype(jnp.float32)
        l1 = l - l0
        pad = jnp.zeros((STAT_ROWS - 5, QROWS), jnp.float32)
        stats = jnp.concatenate([m0, m1, m2, l0, l1, pad], axis=0).astype(jnp.bfloat16)
        for h in range(HEADS_CORE):
            out_ref[h, :KV_RANK] = whole[:, h * ROWS : (h + 1) * ROWS]
            out_ref[h, KV_RANK:] = stats[:, h * ROWS : (h + 1) * ROWS]


def attend(where, keys, q, state):
    state_shapes = (
        jax.ShapeDtypeStruct((TILES, KV_RANK, QTILE), jnp.float32),
        jax.ShapeDtypeStruct((TILES, 1, QTILE), jnp.float32),
        jax.ShapeDtypeStruct((TILES, 1, QTILE), jnp.float32),
    )
    first = state is None
    smem = pl.BlockSpec(memory_space=pltpu.SMEM)
    vmem = pl.BlockSpec(memory_space=pltpu.VMEM)
    scratch = [
        pltpu.VMEM((CHUNK * OWN, 3 * LANES), jnp.bfloat16),
        pltpu.VMEM((KV_RANK, CHUNK * OWN), jnp.bfloat16),
    ]
    if not first:
        scratch = [pltpu.VMEM(s.shape, s.dtype) for s in state_shapes] + scratch
    out_shape = (
        state_shapes
        if first
        else jax.ShapeDtypeStruct((HEADS_CORE, KV_RANK + STAT_ROWS, ROWS), jnp.bfloat16)
    )
    operands = (where, keys, q) + (() if first else tuple(state))
    flops = 2 * QROWS * SOURCES * OWN * (3 * LANES + KV_RANK)
    return pl.pallas_call(
        functools.partial(attend_body, first=first, last=not first),
        out_shape=out_shape,
        in_specs=[smem] + [vmem] * (len(operands) - 1),
        out_specs=jax.tree.map(lambda _: vmem, out_shape),
        scratch_shapes=scratch,
        cost_estimate=pl.CostEstimate(
            flops=flops, transcendentals=QROWS * SOURCES * OWN, bytes_accessed=6000000
        ),
        name="attend_first" if first else "attend_last",
    )(*operands)


def layer(
    inputs,
    norm_gain,
    latent_down,
    rope_down,
    latent_gain,
    mla_query,
    key_up,
    value_up,
    swa_query,
    swa_key,
    swa_value,
    sink_logits,
    out_mla,
    out_swa,
):
    own_rows = inputs.shape[0]
    x_rank = lax.axis_index("x")
    c_rank = lax.axis_index("c")
    tp_rank = lax.axis_index(TP)
    block = lax.axis_index(SP)
    offset = block * ROWS
    own_pos = offset + tp_rank * own_rows + jnp.arange(own_rows, dtype=jnp.int32)
    block_pos = offset + jnp.arange(ROWS, dtype=jnp.int32)
    heads_swa = swa_query.shape[1] // HEAD

    x_count = lax.axis_size("x")

    def in_place(tiles):
        tiles = tiles.reshape(2, x_count, own_rows, -1)
        rows = []
        for x in range(x_count):
            both = lax.dynamic_index_in_dim(tiles, (x_rank - x) % x_count, 1, keepdims=False)
            rows.append(lax.dynamic_index_in_dim(both, c_rank, 0, keepdims=False))
            rows.append(lax.dynamic_index_in_dim(both, 1 - c_rank, 0, keepdims=False))
        return jnp.concatenate(rows, axis=0)

    down = jnp.concatenate([latent_down, rope_down], axis=1)
    width = down.shape[1] // lax.axis_size(TP)
    down = lax.dynamic_slice_in_dim(down, tp_rank * width, width, 1)
    half = down.shape[0] // 2
    fill = ((0, 0), (0, LANES // 2 - width))
    down = jnp.concatenate([jnp.pad(down[:half], fill), jnp.pad(down[half:], fill)], axis=1)
    down = to_everyone(down, SP)
    down = jnp.stack([down[:, :, :width], down[:, :, LANES // 2 : LANES // 2 + width]], axis=1)
    down = down.reshape(-1, width)

    normed = norm_rows(inputs, norm_gain)
    mine = [normed] + [from_x(normed, k) for k in range(1, x_count)]
    mine = jnp.concatenate(mine, axis=0)
    other = from_core(mine)
    pieces = jnp.concatenate([mine, other], axis=0)

    latent = jnp.dot(pieces, down, preferred_element_type=jnp.float32).astype(jnp.bfloat16)
    latent = in_place(latent)
    kv_weights = jnp.concatenate([swa_key, swa_value], axis=1)
    swa_kv = jnp.dot(pieces, kv_weights, preferred_element_type=jnp.float32).astype(jnp.bfloat16)
    swa_kv = in_place(swa_kv)
    count = lax.axis_size(SP)
    before = lax.ppermute(swa_kv[ROWS - WINDOW :], SP, [(i, i + 1) for i in range(count - 1)])
    latent = exchange(latent.reshape(-1, own_rows, width), TP)
    latent = jnp.transpose(latent, (1, 0, 2)).reshape(own_rows, KV_RANK + ROPE)
    keys_latent = norm_rows(latent[:, :KV_RANK], latent_gain)
    keys_rope = rotate(latent[:, KV_RANK:], own_pos)
    packed = jnp.concatenate(
        [
            keys_latent[:, :LANES],
            keys_latent[:, LANES:],
            jnp.concatenate([keys_rope[:16], keys_rope[16:32]], axis=1),
            jnp.concatenate([keys_rope[32:], jnp.zeros((16, ROPE), jnp.bfloat16)], axis=1),
        ],
        axis=0,
    )
    packed, pieces, before = lax.optimization_barrier((packed, pieces, before))
    keys_own = to_everyone(packed, SP)

    queries = jnp.dot(pieces, mla_query, preferred_element_type=jnp.float32)
    queries = in_place(queries.astype(jnp.bfloat16))
    query = jnp.concatenate(
        [
            queries[:, :NOPE],
            rotate(queries[:, NOPE:], block_pos),
            jnp.zeros((ROWS, LANES - ROPE), jnp.bfloat16),
        ],
        axis=1,
    )
    around = jnp.stack([query] + [from_x(query, k) for k in range(1, x_count)], axis=0)
    q_heads = []
    for j in range(HEADS_CORE):
        q_j = lax.dynamic_index_in_dim(around, (x_rank - j) % x_count, 0, keepdims=False)
        up = lax.dynamic_slice_in_dim(key_up, (2 * j + c_rank) * NOPE, NOPE, 1)
        lat = lax.dot_general(
            q_j[:, :NOPE], up, (((1,), (1,)), ((), ())), preferred_element_type=jnp.float32
        ).astype(jnp.bfloat16)
        q_heads.append(jnp.concatenate([lat, q_j[:, NOPE:]], axis=1))
    q_all = jnp.concatenate(q_heads, axis=0)

    swa_q = jnp.dot(pieces, swa_query, preferred_element_type=jnp.float32)
    swa_q = in_place(swa_q.astype(jnp.bfloat16))
    window = jnp.concatenate([before, swa_kv], axis=0)
    window_keys, window_values = window[:, :HEAD], window[:, HEAD:]
    scores = jnp.einsum(
        "tgd,sd->gts",
        swa_q.reshape(ROWS, heads_swa, HEAD),
        window_keys,
        preferred_element_type=jnp.float32,
    ) * HEAD ** (-0.5)
    key_pos = offset - WINDOW + jnp.arange(WINDOW + ROWS, dtype=jnp.int32)
    distance = block_pos[:, None] - key_pos[None, :]
    allowed = (distance >= 0) & (distance < WINDOW) & (key_pos[None, :] >= 0)
    scores = jnp.where(allowed, scores, MASKED_VALUE)
    sink = lax.dynamic_slice_in_dim(sink_logits, tp_rank * heads_swa, heads_swa, 0)
    sink = sink.reshape(heads_swa, 1, 1)
    row_max = jnp.maximum(jnp.max(scores, axis=-1, keepdims=True), sink)
    raw = jnp.exp(scores - row_max)
    weights = (
        raw / (jnp.sum(raw, axis=-1, keepdims=True) + jnp.exp(sink - row_max))
    ).astype(jnp.bfloat16)
    swa_out = jnp.einsum("gts,sd->tgd", weights, window_values, preferred_element_type=jnp.float32)
    swa_out = swa_out.astype(jnp.bfloat16).reshape(ROWS, heads_swa * HEAD)
    swa_x = jnp.stack([swa_out] + [from_x(swa_out, k) for k in range(1, x_count)], axis=0)
    swa_both = jnp.stack([swa_x, from_core(swa_x)], axis=0)
    from_swa = jnp.zeros((ROWS, out_swa.shape[1]), jnp.float32)
    for o in range(2):
        for k in range(x_count):
            head = (2 * ((x_rank - k) % x_count)) + (c_rank + o) % 2
            w = lax.dynamic_slice_in_dim(out_swa, head * 2 * HEAD, 2 * HEAD, 0)
            from_swa += jnp.dot(swa_both[o, k], w, preferred_element_type=jnp.float32)

    keys_own, q_all, from_swa = lax.optimization_barrier((keys_own, q_all, from_swa))
    keys_other = from_core(keys_own)
    rank_own = jnp.stack([block, tp_rank]).astype(jnp.int32)
    rank_other = jnp.stack([block, tp_rank + 1 - 2 * c_rank]).astype(jnp.int32)
    state = attend(rank_own, keys_own, q_all, None)
    partial = attend(rank_other, keys_other, q_all, state)
    parts = exchange(partial, "x").astype(jnp.float32)
    stats = parts[:, KV_RANK:]
    m = stats[:, 0] + stats[:, 1] + stats[:, 2]
    l = stats[:, 3] + stats[:, 4]
    w = jnp.exp2((m - jnp.max(m, axis=0)) * EXP_SCALE)
    denominator = jnp.sum(l * w, axis=0)
    weighted = jnp.sum(parts[:, :KV_RANK] * w[:, None], axis=0)
    latent_out = (weighted / denominator).astype(jnp.bfloat16)
    up = lax.dynamic_slice_in_dim(value_up, tp_rank * VDIM, VDIM, 1)
    mla_out = lax.dot_general(
        latent_out, up, (((0,), (0,)), ((), ())), preferred_element_type=jnp.float32
    ).astype(jnp.bfloat16)
    all_mla = to_everyone(mla_out, TP)
    from_mla = jnp.einsum(
        "rtd,rdn->tn", all_mla, out_mla.reshape(8, -1, 256), preferred_element_type=jnp.float32
    )
    return (from_mla + from_swa).astype(jnp.bfloat16)


def solution(mesh):
    split = Mesh(mesh.devices.reshape(8, 8, 4, 2), SP_TP)
    placed = (
        P(SP_TP, None),
        P(),
        P(SP, None),
        P(SP, None),
        P(),
        P(None, TP),
        P(),
        P(),
        P(None, TP),
        P(None, TP),
        P(None, TP),
        P(),
        P(None, TP),
        P(None, TP),
    )
    return jax.shard_map(layer, mesh=split, in_specs=placed, out_specs=P(SP, TP), check_vma=False)
```

```python
import functools
import math

import jax
import jax.numpy as jnp
from jax import lax
from jax.experimental import pallas as pl
from jax.experimental.pallas import tpu as pltpu
from jax.sharding import Mesh
from jax.sharding import PartitionSpec as P


NOPE = 128
ROPE = 64
VDIM = 128
KV_RANK = 256
HEAD = 64
WINDOW = 128
SP = ("z", "y")
TP = ("x", "c")
SP_TP = ("z", "y", "x", "c")

NORM_EPS = 1e-06
ROPE_BASE = 10000.0
MASKED_VALUE = -1e30
LANES = 128
OWN = 48
SOURCES = 64
ROWS = 384
CHUNK = 16
QTILE = 512
HEADS_CORE = 4
QROWS = HEADS_CORE * ROWS
TILES = QROWS // QTILE
STAT_ROWS = 16
EXP_SCALE = (NOPE + ROPE) ** (-0.5) * math.log2(math.e)


def exchange(array, axis):
    return lax.all_to_all(array, axis, split_axis=0, concat_axis=0, tiled=True)


def to_everyone(array, axis):
    copies = jnp.broadcast_to(array, (lax.axis_size(axis), *array.shape))
    return exchange(copies, axis)


def from_core(value):
    return lax.ppermute(value, "c", [(0, 1), (1, 0)])


def from_x(value, step):
    count = lax.axis_size("x")
    return lax.ppermute(value, "x", [(i, (i + step) % count) for i in range(count)])


def to_float(values):
    return lax.optimization_barrier(values).astype(jnp.float32)


def norm_rows(values, gains):
    widened = to_float(values)
    scaled = widened * lax.rsqrt(jnp.mean(widened * widened, axis=-1, keepdims=True) + NORM_EPS)
    return (scaled * gains).astype(jnp.bfloat16)


def rotate(values, positions):
    full_width = values.shape[-1]
    half_width = full_width // 2
    inverse = ROPE_BASE ** (-jnp.arange(0, full_width, 2, dtype=jnp.float32) / full_width)
    angles = positions.astype(jnp.float32)[:, None] * inverse[None, :]
    cos_table = jnp.cos(angles)
    sin_table = jnp.sin(angles)
    widened = to_float(values)
    first_half = widened[..., :half_width]
    second_half = widened[..., half_width:]
    return jnp.concatenate(
        [
            first_half * cos_table - second_half * sin_table,
            first_half * sin_table + second_half * cos_table,
        ],
        axis=-1,
    ).astype(jnp.bfloat16)


def attend_body(where_ref, keys_ref, *refs, first, last):
    if first:
        (sent_ref, up_ref, o_ref, m_ref, l_ref, q_ref, kc_ref) = refs
        for h in range(HEADS_CORE):
            rows = pl.ds(h * ROWS, ROWS)
            q_ref[rows, :KV_RANK] = lax.dot_general(
                sent_ref[h, :, :NOPE],
                up_ref[h],
                (((1,), (1,)), ((), ())),
                preferred_element_type=jnp.float32,
            ).astype(jnp.bfloat16)
            q_ref[rows, KV_RANK:] = sent_ref[h, :, NOPE : 2 * LANES]
    elif last:
        (q_ref, o_in, m_in, l_in, out_ref, o_ref, m_ref, l_ref, kc_ref) = refs
    block = where_ref[0]
    key_rank = where_ref[1]
    if first:
        o_ref[...] = jnp.zeros_like(o_ref)
        m_ref[...] = jnp.full(m_ref.shape, MASKED_VALUE, jnp.float32)
        l_ref[...] = jnp.zeros_like(l_ref)
    else:
        o_ref[...] = o_in[...]
        m_ref[...] = m_in[...]
        l_ref[...] = l_in[...]
    n_keys = CHUNK * OWN

    def chunk_step(index, masked):
        part = keys_ref[pl.ds(index * CHUNK, CHUNK)]
        k0 = part[:, :OWN].reshape(n_keys, LANES)
        k1 = part[:, OWN : 2 * OWN].reshape(n_keys, LANES)
        tail = part[:, 2 * OWN :]
        turned = jnp.concatenate([tail[..., ROPE:], tail[..., :ROPE]], axis=-1)
        kr = jnp.concatenate([tail, turned], axis=1).reshape(n_keys, LANES)
        kc_ref[:, :LANES] = k0
        kc_ref[:, LANES : 2 * LANES] = k1
        kc_ref[:, 2 * LANES :] = kr
        if masked:
            row = lax.broadcasted_iota(jnp.int32, (n_keys, 1), 0)
            key_pos = (index * CHUNK + row // OWN) * ROWS + key_rank * OWN + row % OWN

        def scores_of(tile):
            return lax.dot_general(
                kc_ref[...],
                q_ref[tile * QTILE : (tile + 1) * QTILE],
                (((1,), (1,)), ((), ())),
                preferred_element_type=jnp.float32,
            )

        def absorb(tile, s):
            if masked:
                col = tile * QTILE + lax.broadcasted_iota(jnp.int32, (1, QTILE), 1)
                allowed = key_pos <= block * ROWS + col % ROWS
                s = jnp.where(allowed, s, MASKED_VALUE)
            old = m_ref[tile]
            new = jnp.maximum(old, jnp.max(s, axis=0, keepdims=True))
            p = jnp.exp2((s - new) * EXP_SCALE)
            if masked:
                p = jnp.where(allowed, p, 0.0)
            alpha = jnp.exp2((old - new) * EXP_SCALE)
            m_ref[tile] = new
            l_ref[tile] = l_ref[tile] * alpha + jnp.sum(p, axis=0, keepdims=True)
            o_ref[tile] = o_ref[tile] * alpha + lax.dot_general(
                kc_ref[:, : 2 * LANES], p.astype(jnp.bfloat16), (((0,), (0,)), ((), ())), preferred_element_type=jnp.float32
            )

        s = scores_of(0)
        for tile in range(TILES):
            ahead = scores_of(tile + 1) if tile + 1 < TILES else None
            absorb(tile, s)
            s = ahead

    def full_step(index, carry):
        chunk_step(index, False)
        return carry

    n_full = block // CHUNK
    lax.fori_loop(0, n_full, full_step, 0)
    chunk_step(n_full, True)
    if last:
        whole = jnp.concatenate([o_ref[t] for t in range(TILES)], axis=1).astype(jnp.bfloat16)
        m = jnp.concatenate([m_ref[t] for t in range(TILES)], axis=1)
        l = jnp.concatenate([l_ref[t] for t in range(TILES)], axis=1)
        m0 = m.astype(jnp.bfloat16).astype(jnp.float32)
        m1 = (m - m0).astype(jnp.bfloat16).astype(jnp.float32)
        m2 = m - m0 - m1
        l0 = l.astype(jnp.bfloat16).astype(jnp.float32)
        l1 = l - l0
        pad = jnp.zeros((STAT_ROWS - 5, QROWS), jnp.float32)
        stats = jnp.concatenate([m0, m1, m2, l0, l1, pad], axis=0).astype(jnp.bfloat16)
        for h in range(HEADS_CORE):
            out_ref[h, :KV_RANK] = whole[:, h * ROWS : (h + 1) * ROWS]
            out_ref[h, KV_RANK:] = stats[:, h * ROWS : (h + 1) * ROWS]


def attend(where, keys, queries, state):
    state_shapes = (
        jax.ShapeDtypeStruct((TILES, KV_RANK, QTILE), jnp.float32),
        jax.ShapeDtypeStruct((TILES, 1, QTILE), jnp.float32),
        jax.ShapeDtypeStruct((TILES, 1, QTILE), jnp.float32),
    )
    first = state is None
    smem = pl.BlockSpec(memory_space=pltpu.SMEM)
    vmem = pl.BlockSpec(memory_space=pltpu.VMEM)
    scratch = [pltpu.VMEM((CHUNK * OWN, 3 * LANES), jnp.bfloat16)]
    if first:
        out_shape = (*state_shapes, jax.ShapeDtypeStruct((QROWS, 3 * LANES), jnp.bfloat16))
        operands = (where, keys, *queries)
    else:
        out_shape = jax.ShapeDtypeStruct((HEADS_CORE, KV_RANK + STAT_ROWS, ROWS), jnp.bfloat16)
        operands = (where, keys, queries, *state)
        scratch = [pltpu.VMEM(s.shape, s.dtype) for s in state_shapes] + scratch
    flops = 2 * QROWS * SOURCES * OWN * (3 * LANES + KV_RANK)
    return pl.pallas_call(
        functools.partial(attend_body, first=first, last=not first),
        out_shape=out_shape,
        in_specs=[smem] + [vmem] * (len(operands) - 1),
        out_specs=jax.tree.map(lambda _: vmem, out_shape),
        scratch_shapes=scratch,
        cost_estimate=pl.CostEstimate(
            flops=flops, transcendentals=QROWS * SOURCES * OWN, bytes_accessed=6000000
        ),
        name="attend_first" if first else "attend_last",
    )(*operands)


def layer(
    inputs,
    norm_gain,
    latent_down,
    rope_down,
    latent_gain,
    mla_query,
    key_up,
    value_up,
    swa_query,
    swa_key,
    swa_value,
    sink_logits,
    out_mla,
    out_swa,
):
    own_rows = inputs.shape[0]
    x_rank = lax.axis_index("x")
    c_rank = lax.axis_index("c")
    tp_rank = lax.axis_index(TP)
    block = lax.axis_index(SP)
    offset = block * ROWS
    own_pos = offset + tp_rank * own_rows + jnp.arange(own_rows, dtype=jnp.int32)
    block_pos = offset + jnp.arange(ROWS, dtype=jnp.int32)
    heads_swa = swa_query.shape[1] // HEAD

    x_count = lax.axis_size("x")

    def by_x(values):
        placed = jnp.zeros((x_count, *values.shape), values.dtype)
        arrived = [values] + [from_x(values, k) for k in range(1, x_count)]
        for k, value in enumerate(arrived):
            at = (x_rank - k) % x_count
            placed = lax.dynamic_update_index_in_dim(placed, value, at, 0)
        return placed

    def by_core(values):
        return tuple(
            lax.dynamic_index_in_dim(values, rank, 0, keepdims=False)
            for rank in (c_rank, 1 - c_rank)
        )

    down = jnp.concatenate([latent_down, rope_down], axis=1)
    width = down.shape[1] // x_count
    down = lax.dynamic_slice_in_dim(down, x_rank * width, width, 1)
    rest = LANES - width
    low, high = (down[:16], down[16:])
    bottom = jnp.concatenate([high[:8, rest:], high[8:, rest:]], axis=1)
    bottom = jnp.pad(bottom, ((0, 0), (0, LANES - bottom.shape[1])))
    down = jnp.concatenate([jnp.concatenate([low, high[:, :rest]], axis=1), bottom], axis=0)
    down = to_everyone(down, SP)
    left = width - rest
    ends = jnp.concatenate([down[:, 16:, :left], down[:, 16:, left : 2 * left]], axis=1)
    high = jnp.concatenate([down[:, :16, width:], ends], axis=2)
    down = jnp.stack([down[:, :16, :width], high], axis=1).reshape(-1, width)

    normed = norm_rows(inputs, norm_gain)
    kv_weights = jnp.concatenate([swa_key, swa_value], axis=1)
    mine = by_x(normed)
    mine = lax.optimization_barrier(mine)
    kv_weights_other = from_core(kv_weights)

    latent = jnp.dot(mine.reshape(-1, mine.shape[2]), down, preferred_element_type=jnp.float32)
    latent = latent.astype(jnp.bfloat16).reshape(x_count, own_rows, width)
    latent = exchange(latent, "x")
    tail_rows = mine[x_count // 2 :].reshape(2 * own_rows, -1)
    tail = jnp.concatenate(
        [
            jnp.dot(tail_rows, weights, preferred_element_type=jnp.float32)
            for weights in (kv_weights, kv_weights_other)
        ],
        axis=1,
    ).astype(jnp.bfloat16)
    count = lax.axis_size(SP)
    before = lax.ppermute(tail, SP, [(i, i + 1) for i in range(count - 1)])
    latent = jnp.transpose(latent, (1, 0, 2)).reshape(own_rows, KV_RANK + ROPE)
    keys_latent = norm_rows(latent[:, :KV_RANK], latent_gain)
    keys_rope = rotate(latent[:, KV_RANK:], own_pos)
    packed = jnp.concatenate(
        [
            keys_latent[:, :LANES],
            keys_latent[:, LANES:],
            jnp.concatenate([keys_rope[: OWN // 2], keys_rope[OWN // 2 :]], axis=1),
        ],
        axis=0,
    )
    packed, mine, before = lax.optimization_barrier((packed, mine, before))
    keys_own = to_everyone(packed, SP)

    other = from_core(mine)
    pieces = jnp.zeros((x_count, 2, *mine.shape[1:]), jnp.bfloat16)
    pieces = lax.dynamic_update_index_in_dim(pieces, mine, c_rank, 1)
    pieces = lax.dynamic_update_index_in_dim(pieces, other, 1 - c_rank, 1)
    pieces = pieces.reshape(ROWS, -1)
    before_other = from_core(before[:, LANES:])
    swa_kv = jnp.dot(pieces, kv_weights, preferred_element_type=jnp.float32)
    swa_kv = swa_kv.astype(jnp.bfloat16)
    before_both = jnp.stack([before[:, :LANES], before_other])
    rows_0, rows_1 = by_core(before_both)
    before = jnp.concatenate([rows_1[3 * OWN - WINDOW : OWN], rows_0[OWN:], rows_1[OWN:]], axis=0)

    queries = jnp.dot(pieces, mla_query, preferred_element_type=jnp.float32)
    queries = queries.astype(jnp.bfloat16)
    query = jnp.concatenate(
        [
            queries[:, :NOPE],
            rotate(queries[:, NOPE:], block_pos),
            jnp.zeros((ROWS, LANES - ROPE), jnp.bfloat16),
        ],
        axis=1,
    )

    swa_q = jnp.dot(pieces, swa_query, preferred_element_type=jnp.float32)
    swa_q = swa_q.astype(jnp.bfloat16)
    window = jnp.concatenate([before, swa_kv], axis=0)
    window_keys, window_values = window[:, :HEAD], window[:, HEAD:]
    scores = jnp.einsum(
        "tgd,sd->gts",
        swa_q.reshape(ROWS, heads_swa, HEAD),
        window_keys,
        preferred_element_type=jnp.float32,
    ) * HEAD ** (-0.5)
    key_pos = offset - WINDOW + jnp.arange(WINDOW + ROWS, dtype=jnp.int32)
    distance = block_pos[:, None] - key_pos[None, :]
    allowed = (distance >= 0) & (distance < WINDOW) & (key_pos[None, :] >= 0)
    scores = jnp.where(allowed, scores, MASKED_VALUE)
    sink = lax.dynamic_slice_in_dim(sink_logits, tp_rank * heads_swa, heads_swa, 0)
    sink = sink.reshape(heads_swa, 1, 1)
    row_max = jnp.maximum(jnp.max(scores, axis=-1, keepdims=True), sink)
    raw = jnp.exp(scores - row_max)
    weights = (
        raw / (jnp.sum(raw, axis=-1, keepdims=True) + jnp.exp(sink - row_max))
    ).astype(jnp.bfloat16)
    swa_out = jnp.einsum("gts,sd->tgd", weights, window_values, preferred_element_type=jnp.float32)
    swa_out = swa_out.astype(jnp.bfloat16).reshape(ROWS, heads_swa * HEAD)
    sent = jnp.concatenate([query, swa_out], axis=1)
    sent = by_x(sent)
    swa_x = sent[:, :, 2 * LANES :]
    up_heads = lax.dynamic_index_in_dim(
        key_up.reshape(KV_RANK, x_count, 2, NOPE), c_rank, 2, keepdims=False
    )
    up_heads = jnp.transpose(up_heads, (1, 0, 2))
    keys_own, sent, up_heads, swa_x = lax.optimization_barrier((keys_own, sent, up_heads, swa_x))
    keys_other = from_core(keys_own)
    swa_other = from_core(swa_x)
    rank_own = jnp.stack([block, tp_rank]).astype(jnp.int32)
    rank_other = jnp.stack([block, tp_rank + 1 - 2 * c_rank]).astype(jnp.int32)
    *state, q_all = attend(rank_own, keys_own, (sent, up_heads), None)
    partial = attend(rank_other, keys_other, q_all, state)
    parts = exchange(partial, "x")
    per_head = out_swa.reshape(x_count, 2, 2 * HEAD, -1)
    from_swa = jnp.zeros((ROWS, out_swa.shape[1]), jnp.float32)
    for values, core in ((swa_x, c_rank), (swa_other, 1 - c_rank)):
        weights = lax.dynamic_index_in_dim(per_head, core, 1, keepdims=False)
        for x in range(x_count):
            from_swa += jnp.dot(values[x], weights[x], preferred_element_type=jnp.float32)
    parts = parts.astype(jnp.float32)
    stats = parts[:, KV_RANK:]
    m = stats[:, 0] + stats[:, 1] + stats[:, 2]
    l = stats[:, 3] + stats[:, 4]
    w = jnp.exp2((m - jnp.max(m, axis=0)) * EXP_SCALE)
    denominator = jnp.sum(l * w, axis=0)
    weighted = jnp.sum(parts[:, :KV_RANK] * w[:, None], axis=0)
    latent_out = (weighted / denominator).astype(jnp.bfloat16)
    up = lax.dynamic_slice_in_dim(value_up, tp_rank * VDIM, VDIM, 1)
    mla_out = lax.dot_general(
        latent_out, up, (((0,), (0,)), ((), ())), preferred_element_type=jnp.float32
    ).astype(jnp.bfloat16)
    all_mla = to_everyone(mla_out, TP)
    from_mla = jnp.einsum(
        "rtd,rdn->tn", all_mla, out_mla.reshape(8, -1, 256), preferred_element_type=jnp.float32
    )
    return (from_mla + from_swa).astype(jnp.bfloat16)


def solution(mesh):
    split = Mesh(mesh.devices.reshape(8, 8, 4, 2), SP_TP)
    placed = (
        P(SP_TP, None),
        P(),
        P(SP, None),
        P(SP, None),
        P(),
        P(None, TP),
        P(),
        P(),
        P(None, TP),
        P(None, TP),
        P(None, TP),
        P(),
        P(None, TP),
        P(None, TP),
    )
    return jax.shard_map(layer, mesh=split, in_specs=placed, out_specs=P(SP, TP), check_vma=False)
```

```python
import functools
import math

import jax
import jax.numpy as jnp
from jax import lax
from jax.experimental import pallas as pl
from jax.experimental.pallas import tpu as pltpu
from jax.sharding import Mesh
from jax.sharding import PartitionSpec as P


NOPE = 128
ROPE = 64
VDIM = 128
KV_RANK = 256
HEAD = 64
WINDOW = 128
SP = ("z", "yh", "yl")
Y = ("yh", "yl")
SAME_PARITY = ("z", "yh")
TP = ("x", "c")
SP_TP = ("z", "yh", "yl", "x", "c")

NORM_EPS = 1e-06
ROPE_BASE = 10000.0
MASKED_VALUE = -1e30
LANES = 128
OWN = 48
SOURCES = 64
ROWS = 384
CHUNK = 16
QTILE = 512
HEADS_CORE = 4
QROWS = HEADS_CORE * ROWS
TILES = QROWS // QTILE
STAT_ROWS = 16
EXP_SCALE = (NOPE + ROPE) ** (-0.5) * math.log2(math.e)


def exchange(array, axis):
    return lax.all_to_all(array, axis, split_axis=0, concat_axis=0, tiled=True)


def to_everyone(array, axis):
    copies = jnp.broadcast_to(array, (lax.axis_size(axis), *array.shape))
    return exchange(copies, axis)


def from_core(value):
    return lax.ppermute(value, "c", [(0, 1), (1, 0)])


def from_x(value, step):
    count = lax.axis_size("x")
    return lax.ppermute(value, "x", [(i, (i + step) % count) for i in range(count)])


def from_y(value, step):
    count = lax.axis_size(Y)
    return lax.ppermute(value, Y, [(i, (i + step) % count) for i in range(count)])


def to_float(values):
    return lax.optimization_barrier(values).astype(jnp.float32)


def norm_rows(values, gains):
    widened = to_float(values)
    scaled = widened * lax.rsqrt(jnp.mean(widened * widened, axis=-1, keepdims=True) + NORM_EPS)
    return (scaled * gains).astype(jnp.bfloat16)


def rotate(values, positions):
    full_width = values.shape[-1]
    half_width = full_width // 2
    inverse = ROPE_BASE ** (-jnp.arange(0, full_width, 2, dtype=jnp.float32) / full_width)
    angles = positions.astype(jnp.float32)[:, None] * inverse[None, :]
    cos_table = jnp.cos(angles)
    sin_table = jnp.sin(angles)
    widened = to_float(values)
    first_half = widened[..., :half_width]
    second_half = widened[..., half_width:]
    return jnp.concatenate(
        [
            first_half * cos_table - second_half * sin_table,
            first_half * sin_table + second_half * cos_table,
        ],
        axis=-1,
    ).astype(jnp.bfloat16)


def attend_body(where_ref, *refs, n_parts, first, last):
    key_refs, refs = refs[:n_parts], refs[n_parts:]
    if first:
        (sent_ref, up_ref, o_ref, m_ref, l_ref, q_ref, kc_ref) = refs
        for h in range(HEADS_CORE):
            rows = pl.ds(h * ROWS, ROWS)
            q_ref[rows, :KV_RANK] = lax.dot_general(
                sent_ref[h, :, :NOPE],
                up_ref[h],
                (((1,), (1,)), ((), ())),
                preferred_element_type=jnp.float32,
            ).astype(jnp.bfloat16)
            q_ref[rows, KV_RANK:] = sent_ref[h, :, NOPE : 2 * LANES]
        o_ref[...] = jnp.zeros_like(o_ref)
        m_ref[...] = jnp.full(m_ref.shape, MASKED_VALUE, jnp.float32)
        l_ref[...] = jnp.zeros_like(l_ref)
    else:
        if last:
            (q_ref, o_in, m_in, l_in, out_ref, o_ref, m_ref, l_ref, kc_ref) = refs
        else:
            (q_ref, o_in, m_in, l_in, o_ref, m_ref, l_ref, kc_ref) = refs
        o_ref[...] = o_in[...]
        m_ref[...] = m_in[...]
        l_ref[...] = l_in[...]
    block = where_ref[0]
    parity = where_ref[1]
    n_keys = CHUNK * OWN

    def load_keys(keys_ref, index):
        part = keys_ref[pl.ds(index * CHUNK, CHUNK)]
        tail = part[:, 2 * OWN :]
        turned = jnp.concatenate([tail[..., ROPE:], tail[..., :ROPE]], axis=-1)
        kc_ref[:, :LANES] = part[:, :OWN].reshape(n_keys, LANES)
        kc_ref[:, LANES : 2 * LANES] = part[:, OWN : 2 * OWN].reshape(n_keys, LANES)
        kc_ref[:, 2 * LANES :] = jnp.concatenate([tail, turned], axis=1).reshape(n_keys, LANES)

    def load_part(part, index):
        if n_parts == 1:
            load_keys(key_refs[0], index)
        for i in range(n_parts if n_parts > 1 else 0):

            @pl.when(part == i)
            def _(i=i):
                load_keys(key_refs[i], index)

    def chunk_step(part, index, masked):
        load_part(part, index)
        if masked:
            row = lax.broadcasted_iota(jnp.int32, (n_keys, 1), 0)
            source = 2 * (index * CHUNK + row // OWN) + parity
            key_pos = source * ROWS + where_ref[2 + part] * OWN + row % OWN

        def scores_of(tile):
            return lax.dot_general(
                kc_ref[...],
                q_ref[tile * QTILE : (tile + 1) * QTILE],
                (((1,), (1,)), ((), ())),
                preferred_element_type=jnp.float32,
            )

        def absorb(tile, s):
            if masked:
                col = tile * QTILE + lax.broadcasted_iota(jnp.int32, (1, QTILE), 1)
                allowed = key_pos <= block * ROWS + col % ROWS
                s = jnp.where(allowed, s, MASKED_VALUE)
            old = m_ref[tile]
            new = jnp.maximum(old, jnp.max(s, axis=0, keepdims=True))
            p = jnp.exp2((s - new) * EXP_SCALE)
            if masked:
                p = jnp.where(allowed, p, 0.0)
            alpha = jnp.exp2((old - new) * EXP_SCALE)
            m_ref[tile] = new
            l_ref[tile] = l_ref[tile] * alpha + jnp.sum(p, axis=0, keepdims=True)
            o_ref[tile] = o_ref[tile] * alpha + lax.dot_general(
                kc_ref[:, : 2 * LANES],
                p.astype(jnp.bfloat16),
                (((0,), (0,)), ((), ())),
                preferred_element_type=jnp.float32,
            )

        s = scores_of(0)
        for tile in range(TILES):
            ahead = scores_of(tile + 1) if tile + 1 < TILES else None
            absorb(tile, s)
            s = ahead

    n_chunks = SOURCES // 2 // CHUNK
    n_full = (block - parity + 1) // (2 * CHUNK)

    def full_step(step, carry):
        if n_parts == 1:
            chunk_step(0, step, False)
        else:
            part = (step >= n_full).astype(jnp.int32)
            chunk_step(part, step - part * n_full, False)
        return carry

    lax.fori_loop(0, n_full * n_parts, full_step, 0)

    @pl.when(n_full < n_chunks)
    def _():
        if n_parts == 1:
            chunk_step(0, n_full, True)
        else:

            def masked_step(part, carry):
                chunk_step(part, n_full, True)
                return carry

            lax.fori_loop(0, n_parts, masked_step, 0)

    if last:
        whole = jnp.concatenate([o_ref[t] for t in range(TILES)], axis=1).astype(jnp.bfloat16)
        m = jnp.concatenate([m_ref[t] for t in range(TILES)], axis=1)
        l = jnp.concatenate([l_ref[t] for t in range(TILES)], axis=1)
        m0 = m.astype(jnp.bfloat16).astype(jnp.float32)
        m1 = (m - m0).astype(jnp.bfloat16).astype(jnp.float32)
        m2 = m - m0 - m1
        l0 = l.astype(jnp.bfloat16).astype(jnp.float32)
        l1 = l - l0
        pad = jnp.zeros((STAT_ROWS - 5, QROWS), jnp.float32)
        stats = jnp.concatenate([m0, m1, m2, l0, l1, pad], axis=0).astype(jnp.bfloat16)
        for h in range(HEADS_CORE):
            out_ref[h, :KV_RANK] = whole[:, h * ROWS : (h + 1) * ROWS]
            out_ref[h, KV_RANK:] = stats[:, h * ROWS : (h + 1) * ROWS]


def attend(where, parts, queries, state, last):
    state_shapes = (
        jax.ShapeDtypeStruct((TILES, KV_RANK, QTILE), jnp.float32),
        jax.ShapeDtypeStruct((TILES, 1, QTILE), jnp.float32),
        jax.ShapeDtypeStruct((TILES, 1, QTILE), jnp.float32),
    )
    first = state is None
    smem = pl.BlockSpec(memory_space=pltpu.SMEM)
    vmem = pl.BlockSpec(memory_space=pltpu.VMEM)
    scratch = [pltpu.VMEM((CHUNK * OWN, 3 * LANES), jnp.bfloat16)]
    out_shape = state_shapes
    if first:
        out_shape = (*state_shapes, jax.ShapeDtypeStruct((QROWS, 3 * LANES), jnp.bfloat16))
        operands = (where, *parts, *queries)
    else:
        operands = (where, *parts, queries, *state)
    if last:
        out_shape = jax.ShapeDtypeStruct((HEADS_CORE, KV_RANK + STAT_ROWS, ROWS), jnp.bfloat16)
        scratch = [pltpu.VMEM(s.shape, s.dtype) for s in state_shapes] + scratch
    n_keys = SOURCES // 2 * OWN * len(parts)
    return pl.pallas_call(
        functools.partial(attend_body, n_parts=len(parts), first=first, last=last),
        out_shape=out_shape,
        in_specs=[smem] + [vmem] * (len(operands) - 1),
        out_specs=jax.tree.map(lambda _: vmem, out_shape),
        scratch_shapes=scratch,
        cost_estimate=pl.CostEstimate(
            flops=2 * QROWS * n_keys * (3 * LANES + KV_RANK),
            transcendentals=QROWS * n_keys,
            bytes_accessed=6000000,
        ),
    )(*operands)


def layer(
    inputs,
    norm_gain,
    latent_down,
    rope_down,
    latent_gain,
    mla_query,
    key_up,
    value_up,
    swa_query,
    swa_key,
    swa_value,
    sink_logits,
    out_mla,
    out_swa,
):
    own_rows = inputs.shape[0]
    x_rank = lax.axis_index("x")
    c_rank = lax.axis_index("c")
    tp_rank = lax.axis_index(TP)
    block = lax.axis_index(SP)
    offset = block * ROWS
    own_pos = offset + tp_rank * own_rows + jnp.arange(own_rows, dtype=jnp.int32)
    block_pos = offset + jnp.arange(ROWS, dtype=jnp.int32)
    heads_swa = swa_query.shape[1] // HEAD

    x_count = lax.axis_size("x")

    def by_x(values):
        placed = jnp.zeros((x_count, *values.shape), values.dtype)
        arrived = [values] + [from_x(values, k) for k in range(1, x_count)]
        for k, value in enumerate(arrived):
            at = (x_rank - k) % x_count
            placed = lax.dynamic_update_index_in_dim(placed, value, at, 0)
        return placed

    half = rope_down.shape[0] // 2
    down = jnp.concatenate(
        [
            latent_down[:, :LANES],
            latent_down[:, LANES:],
            jnp.concatenate([rope_down[:half], rope_down[half:]], axis=1),
        ],
        axis=0,
    )
    down = to_everyone(down, SP)
    rope_tiles = down[:, 4 * half :]
    down_rope = jnp.stack([rope_tiles[:, :, :ROPE], rope_tiles[:, :, ROPE:]], axis=1)
    down_rope = down_rope.reshape(-1, ROPE)
    down_latent = jnp.concatenate([down[:, : 2 * half], down[:, 2 * half : 4 * half]], axis=2)
    down_latent = down_latent.reshape(-1, KV_RANK)

    normed = norm_rows(inputs, norm_gain)
    kv_weights = jnp.concatenate([swa_key, swa_value], axis=1)
    mine = by_x(normed)
    other = from_core(mine)
    pieces = jnp.zeros((x_count, 2, *mine.shape[1:]), jnp.bfloat16)
    pieces = lax.dynamic_update_index_in_dim(pieces, mine, c_rank, 1)
    pieces = lax.dynamic_update_index_in_dim(pieces, other, 1 - c_rank, 1)
    pieces = pieces.reshape(ROWS, -1)
    swa_kv = jnp.dot(pieces, kv_weights, preferred_element_type=jnp.float32)
    swa_kv = swa_kv.astype(jnp.bfloat16)
    count = lax.axis_size(SP)
    before = lax.ppermute(
        swa_kv[ROWS - WINDOW :], SP, [(i, i + 1) for i in range(count - 1)]
    )
    queries = jnp.dot(pieces, mla_query, preferred_element_type=jnp.float32)
    queries = queries.astype(jnp.bfloat16)
    query = jnp.concatenate(
        [
            queries[:, :NOPE],
            rotate(queries[:, NOPE:], block_pos),
            jnp.zeros((ROWS, LANES - ROPE), jnp.bfloat16),
        ],
        axis=1,
    )

    latent = jnp.dot(normed, down_latent, preferred_element_type=jnp.float32)
    rope_raw = jnp.dot(normed, down_rope, preferred_element_type=jnp.float32)
    keys_latent = norm_rows(latent.astype(jnp.bfloat16), latent_gain)
    keys_rope = rotate(rope_raw.astype(jnp.bfloat16), own_pos)
    packed = jnp.concatenate(
        [
            keys_latent[:, :LANES],
            keys_latent[:, LANES:],
            jnp.concatenate([keys_rope[: OWN // 2], keys_rope[OWN // 2 :]], axis=1),
        ],
        axis=0,
    )
    packed, pieces, swa_kv, before = lax.optimization_barrier((packed, pieces, swa_kv, before))
    keys_own = to_everyone(packed, SAME_PARITY)

    swa_q = jnp.dot(pieces, swa_query, preferred_element_type=jnp.float32)
    swa_q = swa_q.astype(jnp.bfloat16)
    window = jnp.concatenate([before, swa_kv], axis=0)
    window_keys, window_values = window[:, :HEAD], window[:, HEAD:]
    scores = jnp.einsum(
        "tgd,sd->gts",
        swa_q.reshape(ROWS, heads_swa, HEAD),
        window_keys,
        preferred_element_type=jnp.float32,
    ) * HEAD ** (-0.5)
    key_pos = offset - WINDOW + jnp.arange(WINDOW + ROWS, dtype=jnp.int32)
    distance = block_pos[:, None] - key_pos[None, :]
    allowed = (distance >= 0) & (distance < WINDOW) & (key_pos[None, :] >= 0)
    scores = jnp.where(allowed, scores, MASKED_VALUE)
    sink = lax.dynamic_slice_in_dim(sink_logits, tp_rank * heads_swa, heads_swa, 0)
    sink = sink.reshape(heads_swa, 1, 1)
    row_max = jnp.maximum(jnp.max(scores, axis=-1, keepdims=True), sink)
    raw = jnp.exp(scores - row_max)
    weights = (
        raw / (jnp.sum(raw, axis=-1, keepdims=True) + jnp.exp(sink - row_max))
    ).astype(jnp.bfloat16)
    swa_out = jnp.einsum("gts,sd->tgd", weights, window_values, preferred_element_type=jnp.float32)
    swa_out = swa_out.astype(jnp.bfloat16).reshape(ROWS, heads_swa * HEAD)
    sent = jnp.concatenate([query, swa_out], axis=1)
    sent = by_x(sent)
    swa_x = sent[:, :, 2 * LANES :]
    swa_other = from_core(swa_x)
    up_heads = jnp.stack(
        [lax.dynamic_slice_in_dim(key_up, (2 * x + c_rank) * NOPE, NOPE, 1) for x in range(x_count)]
    )
    parity = lax.axis_index("yl")
    rank_other = tp_rank + 1 - 2 * c_rank
    where = [
        jnp.stack(entries).astype(jnp.int32)
        for entries in (
            (block, parity, tp_rank),
            (block, parity, rank_other),
            (block, 1 - parity, tp_rank, rank_other),
        )
    ]
    keys_own, sent, up_heads, swa_x, where = lax.optimization_barrier(
        (keys_own, sent, up_heads, swa_x, where)
    )
    half = keys_own.shape[0] // 2
    low = from_y(keys_own[:half], 1)
    high = from_y(keys_own[half:], -1)
    keys_other = from_core(keys_own)
    *state, q_all = attend(where[0], (keys_own,), (sent, up_heads), None, False)
    far_own = jnp.concatenate([low, high], axis=0)
    far_own, state = lax.optimization_barrier((far_own, state))
    far_other = from_core(far_own)
    state = attend(where[1], (keys_other,), q_all, state, False)
    partial = attend(where[2], (far_own, far_other), q_all, state, True)
    parts = exchange(partial, "x")
    per_head = out_swa.reshape(x_count, 2, 2 * HEAD, -1)
    from_swa = jnp.zeros((ROWS, out_swa.shape[1]), jnp.float32)
    for values, core in ((swa_x, c_rank), (swa_other, 1 - c_rank)):
        weights = lax.dynamic_index_in_dim(per_head, core, 1, keepdims=False)
        for x in range(x_count):
            from_swa += jnp.dot(values[x], weights[x], preferred_element_type=jnp.float32)
    parts = parts.astype(jnp.float32)
    stats = parts[:, KV_RANK:]
    m = stats[:, 0] + stats[:, 1] + stats[:, 2]
    l = stats[:, 3] + stats[:, 4]
    w = jnp.exp2((m - jnp.max(m, axis=0)) * EXP_SCALE)
    denominator = jnp.sum(l * w, axis=0)
    weighted = jnp.sum(parts[:, :KV_RANK] * w[:, None], axis=0)
    latent_out = (weighted / denominator).astype(jnp.bfloat16)
    up = lax.dynamic_slice_in_dim(value_up, tp_rank * VDIM, VDIM, 1)
    mla_out = lax.dot_general(
        latent_out, up, (((0,), (0,)), ((), ())), preferred_element_type=jnp.float32
    ).astype(jnp.bfloat16)
    all_mla = to_everyone(mla_out, TP)
    from_mla = jnp.einsum(
        "rtd,rdn->tn", all_mla, out_mla.reshape(8, -1, 256), preferred_element_type=jnp.float32
    )
    return (from_mla + from_swa).astype(jnp.bfloat16)


def solution(mesh):
    split = Mesh(mesh.devices.reshape(8, 4, 2, 4, 2), SP_TP)
    placed = (
        P(SP_TP, None),
        P(),
        P(SP, None),
        P(SP, None),
        P(),
        P(None, TP),
        P(),
        P(),
        P(None, TP),
        P(None, TP),
        P(None, TP),
        P(),
        P(None, TP),
        P(None, TP),
    )
    return jax.shard_map(layer, mesh=split, in_specs=placed, out_specs=P(SP, TP), check_vma=False)
```

```python
import functools
import math

import jax
import jax.numpy as jnp
from jax import lax
from jax.experimental import pallas as pl
from jax.experimental.pallas import tpu as pltpu
from jax.sharding import Mesh
from jax.sharding import PartitionSpec as P


NOPE = 128
ROPE = 64
VDIM = 128
KV_RANK = 256
HEAD = 64
WINDOW = 128
SP = ("z", "yh", "yl")
Y = ("yh", "yl")
SAME_PARITY = ("z", "yh")
TP = ("x", "c")
SP_TP = ("z", "yh", "yl", "x", "c")

NORM_EPS = 1e-06
ROPE_BASE = 10000.0
MASKED_VALUE = -1e30
LANES = 128
OWN = 48
SOURCES = 64
ROWS = 384
CHUNK = 16
QTILE = 512
HEADS_CORE = 4
QROWS = HEADS_CORE * ROWS
TILES = QROWS // QTILE
STAT_ROWS = 16
EXP_SCALE = (NOPE + ROPE) ** (-0.5) * math.log2(math.e)


def exchange(array, axis):
    return lax.all_to_all(array, axis, split_axis=0, concat_axis=0, tiled=True)


def to_everyone(array, axis):
    copies = jnp.broadcast_to(array, (lax.axis_size(axis), *array.shape))
    return exchange(copies, axis)


def from_core(value):
    return lax.ppermute(value, "c", [(0, 1), (1, 0)])


def from_x(value, step):
    count = lax.axis_size("x")
    return lax.ppermute(value, "x", [(i, (i + step) % count) for i in range(count)])


def from_y(value, step):
    count = lax.axis_size(Y)
    return lax.ppermute(value, Y, [(i, (i + step) % count) for i in range(count)])


def to_float(values):
    return lax.optimization_barrier(values).astype(jnp.float32)


def norm_rows(values, gains):
    widened = to_float(values)
    scaled = widened * lax.rsqrt(jnp.mean(widened * widened, axis=-1, keepdims=True) + NORM_EPS)
    return (scaled * gains).astype(jnp.bfloat16)


def rotate(values, positions):
    full_width = values.shape[-1]
    half_width = full_width // 2
    inverse = ROPE_BASE ** (-jnp.arange(0, full_width, 2, dtype=jnp.float32) / full_width)
    angles = positions.astype(jnp.float32)[:, None] * inverse[None, :]
    cos_table = jnp.cos(angles)
    sin_table = jnp.sin(angles)
    widened = to_float(values)
    first_half = widened[..., :half_width]
    second_half = widened[..., half_width:]
    return jnp.concatenate(
        [
            first_half * cos_table - second_half * sin_table,
            first_half * sin_table + second_half * cos_table,
        ],
        axis=-1,
    ).astype(jnp.bfloat16)


def attend_body(where_ref, *refs, n_parts, first, last):
    key_refs, refs = refs[:n_parts], refs[n_parts:]
    if first:
        (sent_ref, up_ref, o_ref, m_ref, l_ref, q_ref, kc_ref) = refs
        for h in range(HEADS_CORE):
            rows = pl.ds(h * ROWS, ROWS)
            q_ref[rows, :KV_RANK] = lax.dot_general(
                sent_ref[h, :, :NOPE],
                up_ref[h],
                (((1,), (1,)), ((), ())),
                preferred_element_type=jnp.float32,
            ).astype(jnp.bfloat16)
            q_ref[rows, KV_RANK:] = sent_ref[h, :, NOPE : 2 * LANES]
        o_ref[...] = jnp.zeros_like(o_ref)
        m_ref[...] = jnp.full(m_ref.shape, MASKED_VALUE, jnp.float32)
        l_ref[...] = jnp.zeros_like(l_ref)
    else:
        if last:
            (q_ref, o_in, m_in, l_in, out_ref, o_ref, m_ref, l_ref, kc_ref) = refs
        else:
            (q_ref, o_in, m_in, l_in, o_ref, m_ref, l_ref, kc_ref) = refs
        o_ref[...] = o_in[...]
        m_ref[...] = m_in[...]
        l_ref[...] = l_in[...]
    block = where_ref[0]
    parity = where_ref[1]
    n_keys = CHUNK * OWN

    def load_keys(keys_ref, index):
        part = keys_ref[pl.ds(index * CHUNK, CHUNK)]
        tail = part[:, 2 * OWN :]
        turned = jnp.concatenate([tail[..., ROPE:], tail[..., :ROPE]], axis=-1)
        kc_ref[:, :LANES] = part[:, :OWN].reshape(n_keys, LANES)
        kc_ref[:, LANES : 2 * LANES] = part[:, OWN : 2 * OWN].reshape(n_keys, LANES)
        kc_ref[:, 2 * LANES :] = jnp.concatenate([tail, turned], axis=1).reshape(n_keys, LANES)

    def load_part(part, index):
        if n_parts == 1:
            load_keys(key_refs[0], index)
        for i in range(n_parts if n_parts > 1 else 0):

            @pl.when(part == i)
            def _(i=i):
                load_keys(key_refs[i], index)

    def chunk_step(part, index, masked):
        load_part(part, index)
        if masked:
            row = lax.broadcasted_iota(jnp.int32, (n_keys, 1), 0)
            source = 2 * (index * CHUNK + row // OWN) + parity
            key_pos = source * ROWS + where_ref[2 + part] * OWN + row % OWN

        def scores_of(tile):
            return lax.dot_general(
                kc_ref[...],
                q_ref[tile * QTILE : (tile + 1) * QTILE],
                (((1,), (1,)), ((), ())),
                preferred_element_type=jnp.float32,
            )

        def absorb(tile, s):
            if masked:
                col = tile * QTILE + lax.broadcasted_iota(jnp.int32, (1, QTILE), 1)
                allowed = key_pos <= block * ROWS + col % ROWS
                s = jnp.where(allowed, s, MASKED_VALUE)
            old = m_ref[tile]
            new = jnp.maximum(old, jnp.max(s, axis=0, keepdims=True))
            p = jnp.exp2((s - new) * EXP_SCALE)
            if masked:
                p = jnp.where(allowed, p, 0.0)
            alpha = jnp.exp2((old - new) * EXP_SCALE)
            m_ref[tile] = new
            l_ref[tile] = l_ref[tile] * alpha + jnp.sum(p, axis=0, keepdims=True)
            o_ref[tile] = o_ref[tile] * alpha + lax.dot_general(
                kc_ref[:, : 2 * LANES],
                p.astype(jnp.bfloat16),
                (((0,), (0,)), ((), ())),
                preferred_element_type=jnp.float32,
            )

        s = scores_of(0)
        for tile in range(TILES):
            ahead = scores_of(tile + 1) if tile + 1 < TILES else None
            absorb(tile, s)
            s = ahead

    n_chunks = SOURCES // 2 // CHUNK
    n_full = (block - parity + 1) // (2 * CHUNK)

    def full_step(step, carry):
        if n_parts == 1:
            chunk_step(0, step, False)
        else:
            part = (step >= n_full).astype(jnp.int32)
            chunk_step(part, step - part * n_full, False)
        return carry

    lax.fori_loop(0, n_full * n_parts, full_step, 0)

    @pl.when(n_full < n_chunks)
    def _():
        if n_parts == 1:
            chunk_step(0, n_full, True)
        else:

            def masked_step(part, carry):
                chunk_step(part, n_full, True)
                return carry

            lax.fori_loop(0, n_parts, masked_step, 0)

    if last:
        whole = jnp.concatenate([o_ref[t] for t in range(TILES)], axis=1).astype(jnp.bfloat16)
        m = jnp.concatenate([m_ref[t] for t in range(TILES)], axis=1)
        l = jnp.concatenate([l_ref[t] for t in range(TILES)], axis=1)
        m0 = m.astype(jnp.bfloat16).astype(jnp.float32)
        m1 = (m - m0).astype(jnp.bfloat16).astype(jnp.float32)
        m2 = m - m0 - m1
        l0 = l.astype(jnp.bfloat16).astype(jnp.float32)
        l1 = l - l0
        pad = jnp.zeros((STAT_ROWS - 5, QROWS), jnp.float32)
        stats = jnp.concatenate([m0, m1, m2, l0, l1, pad], axis=0).astype(jnp.bfloat16)
        for h in range(HEADS_CORE):
            out_ref[h, :KV_RANK] = whole[:, h * ROWS : (h + 1) * ROWS]
            out_ref[h, KV_RANK:] = stats[:, h * ROWS : (h + 1) * ROWS]


def attend(where, parts, queries, state, last):
    state_shapes = (
        pltpu.VMEM((TILES, KV_RANK, QTILE), jnp.float32),
        pltpu.VMEM((TILES, 1, QTILE), jnp.float32),
        pltpu.VMEM((TILES, 1, QTILE), jnp.float32),
    )
    first = state is None
    smem = pl.BlockSpec(memory_space=pltpu.SMEM)
    vmem = pl.BlockSpec(memory_space=pltpu.VMEM)
    scratch = [pltpu.VMEM((CHUNK * OWN, 3 * LANES), jnp.bfloat16)]
    out_shape = state_shapes
    if first:
        out_shape = (*state_shapes, pltpu.VMEM((QROWS, 3 * LANES), jnp.bfloat16))
        operands = (where, *parts, *queries)
    else:
        operands = (where, *parts, queries, *state)
    if last:
        out_shape = jax.ShapeDtypeStruct((HEADS_CORE, KV_RANK + STAT_ROWS, ROWS), jnp.bfloat16)
        scratch = list(state_shapes) + scratch
    if not first:
        operands = operands[: 1 + len(parts)] + tuple(
            pltpu.with_memory_space_constraint(value, pltpu.VMEM)
            for value in operands[1 + len(parts) :]
        )
    n_keys = SOURCES // 2 * OWN * len(parts)
    return pl.pallas_call(
        functools.partial(attend_body, n_parts=len(parts), first=first, last=last),
        out_shape=out_shape,
        in_specs=[smem] + [vmem] * (len(operands) - 1),
        out_specs=jax.tree.map(lambda _: vmem, out_shape),
        scratch_shapes=scratch,
        compiler_params=pltpu.CompilerParams(vmem_limit_bytes=24 * 1024 * 1024),
        cost_estimate=pl.CostEstimate(
            flops=2 * QROWS * n_keys * (3 * LANES + KV_RANK),
            transcendentals=QROWS * n_keys,
            bytes_accessed=6000000,
        ),
    )(*operands)


def joined_body(low_ref, high_ref, out_ref):
    half = low_ref.shape[0]
    out_ref[:half] = low_ref[...]
    out_ref[half:] = high_ref[...]


def joined(low, high):
    vmem = pl.BlockSpec(memory_space=pltpu.VMEM)
    return pl.pallas_call(
        joined_body,
        out_shape=jax.ShapeDtypeStruct((2 * low.shape[0], *low.shape[1:]), low.dtype),
        in_specs=[vmem, vmem],
        out_specs=vmem,
        compiler_params=pltpu.CompilerParams(vmem_limit_bytes=8 * 1024 * 1024),
        name="joined",
    )(low, high)


def windowed_body(where_ref, sink_ref, rows_ref, before_ref, query_ref, out_ref):
    out_ref[:, : 2 * LANES] = query_ref[...]
    for tile in range(ROWS // WINDOW):
        here = rows_ref[tile * WINDOW : (tile + 1) * WINDOW]
        if tile == 0:
            behind = before_ref[...]
        else:
            behind = rows_ref[(tile - 1) * WINDOW : tile * WINDOW, LANES:]
        both = jnp.concatenate([behind, here[:, LANES:]], axis=0)
        row = lax.broadcasted_iota(jnp.int32, (WINDOW, 2 * WINDOW), 0)
        col = lax.broadcasted_iota(jnp.int32, (WINDOW, 2 * WINDOW), 1)
        allowed = (col > row) & (col <= row + WINDOW)
        if tile == 0:
            allowed = allowed & ((col >= WINDOW) | (where_ref[0] > 0))
        outs = []
        for h in range(LANES // HEAD):
            scores = lax.dot_general(
                here[:, h * HEAD : (h + 1) * HEAD],
                both[:, :HEAD],
                (((1,), (1,)), ((), ())),
                preferred_element_type=jnp.float32,
            ) * HEAD ** (-0.5)
            scores = jnp.where(allowed, scores, MASKED_VALUE)
            sink = jnp.full((WINDOW, 1), sink_ref[where_ref[2] * (LANES // HEAD) + h])
            row_max = jnp.maximum(jnp.max(scores, axis=1, keepdims=True), sink)
            raw = jnp.exp(scores - row_max)
            total = jnp.sum(raw, axis=1, keepdims=True) + jnp.exp(sink - row_max)
            weights = (raw / total).astype(jnp.bfloat16)
            outs.append(jnp.dot(weights, both[:, HEAD:], preferred_element_type=jnp.float32))
        out_ref[tile * WINDOW : (tile + 1) * WINDOW, 2 * LANES :] = jnp.concatenate(
            outs, axis=1
        ).astype(jnp.bfloat16)


def windowed(where, sink_logits, rows, before, query):
    smem = pl.BlockSpec(memory_space=pltpu.SMEM)
    vmem = pl.BlockSpec(memory_space=pltpu.VMEM)
    return pl.pallas_call(
        windowed_body,
        out_shape=jax.ShapeDtypeStruct((ROWS, 3 * LANES), jnp.bfloat16),
        in_specs=[smem, smem, vmem, vmem, vmem],
        out_specs=vmem,
        compiler_params=pltpu.CompilerParams(vmem_limit_bytes=16 * 1024 * 1024),
        cost_estimate=pl.CostEstimate(
            flops=4 * ROWS * 2 * WINDOW * LANES,
            transcendentals=ROWS * 4 * WINDOW,
            bytes_accessed=1000000,
        ),
        name="windowed",
    )(where, sink_logits, rows, before, query)


def layer(
    inputs,
    norm_gain,
    latent_down,
    rope_down,
    latent_gain,
    mla_query,
    key_up,
    value_up,
    swa_query,
    swa_key,
    swa_value,
    sink_logits,
    out_mla,
    out_swa,
):
    own_rows = inputs.shape[0]
    x_rank = lax.axis_index("x")
    c_rank = lax.axis_index("c")
    tp_rank = lax.axis_index(TP)
    block = lax.axis_index(SP)
    offset = block * ROWS
    own_pos = offset + tp_rank * own_rows + jnp.arange(own_rows, dtype=jnp.int32)
    block_pos = offset + jnp.arange(ROWS, dtype=jnp.int32)

    x_count = lax.axis_size("x")

    def by_x(values):
        placed = jnp.zeros((x_count, *values.shape), values.dtype)
        arrived = [values] + [from_x(values, k) for k in range(1, x_count)]
        for k, value in enumerate(arrived):
            at = (x_rank - k) % x_count
            placed = lax.dynamic_update_index_in_dim(placed, value, at, 0)
        return placed

    half = rope_down.shape[0] // 2
    down = jnp.concatenate(
        [
            latent_down[:, :LANES],
            latent_down[:, LANES:],
            jnp.concatenate([rope_down[:half], rope_down[half:]], axis=1),
        ],
        axis=0,
    )
    down = to_everyone(down, SP)
    rope_tiles = down[:, 4 * half :]
    down_rope = jnp.stack([rope_tiles[:, :, :ROPE], rope_tiles[:, :, ROPE:]], axis=1)
    down_rope = down_rope.reshape(-1, ROPE)
    down_latent = jnp.concatenate([down[:, : 2 * half], down[:, 2 * half : 4 * half]], axis=2)
    down_latent = down_latent.reshape(-1, KV_RANK)

    normed = norm_rows(inputs, norm_gain)
    swa_weights = jnp.concatenate([swa_query, swa_key, swa_value], axis=1)
    mine = by_x(normed)
    other = from_core(mine)
    pieces = jnp.zeros((x_count, 2, *mine.shape[1:]), jnp.bfloat16)
    pieces = lax.dynamic_update_index_in_dim(pieces, mine, c_rank, 1)
    pieces = lax.dynamic_update_index_in_dim(pieces, other, 1 - c_rank, 1)
    pieces = pieces.reshape(ROWS, -1)
    swa_rows = jnp.dot(pieces, swa_weights, preferred_element_type=jnp.float32)
    swa_rows = swa_rows.astype(jnp.bfloat16)
    count = lax.axis_size(SP)
    before = lax.ppermute(
        swa_rows[ROWS - WINDOW :, LANES:], SP, [(i, i + 1) for i in range(count - 1)]
    )
    queries = jnp.dot(pieces, mla_query, preferred_element_type=jnp.float32)
    queries = queries.astype(jnp.bfloat16)
    query = jnp.concatenate(
        [
            queries[:, :NOPE],
            rotate(queries[:, NOPE:], block_pos),
            jnp.zeros((ROWS, LANES - ROPE), jnp.bfloat16),
        ],
        axis=1,
    )

    latent = jnp.dot(normed, down_latent, preferred_element_type=jnp.float32)
    rope_raw = jnp.dot(normed, down_rope, preferred_element_type=jnp.float32)
    keys_latent = norm_rows(latent.astype(jnp.bfloat16), latent_gain)
    keys_rope = rotate(rope_raw.astype(jnp.bfloat16), own_pos)
    packed = jnp.concatenate(
        [
            keys_latent[:, :LANES],
            keys_latent[:, LANES:],
            jnp.concatenate([keys_rope[: OWN // 2], keys_rope[OWN // 2 :]], axis=1),
        ],
        axis=0,
    )
    up_heads = jnp.stack(
        [lax.dynamic_slice_in_dim(key_up, (2 * x + c_rank) * NOPE, NOPE, 1) for x in range(x_count)]
    )
    parity = lax.axis_index("yl")
    rank_other = tp_rank + 1 - 2 * c_rank
    where = [
        jnp.stack(entries).astype(jnp.int32)
        for entries in (
            (block, parity, tp_rank),
            (block, parity, rank_other),
            (block, 1 - parity, tp_rank, rank_other),
        )
    ]
    packed, swa_rows, before, query, up_heads, where = lax.optimization_barrier(
        (packed, swa_rows, before, query, up_heads, where)
    )
    keys_own = to_everyone(packed, SAME_PARITY)

    sent = windowed(where[0], sink_logits, swa_rows, before, query)
    sent = by_x(sent)
    swa_x = sent[:, :, 2 * LANES :]
    swa_other = from_core(swa_x)
    keys_own, sent, up_heads, swa_x, where = lax.optimization_barrier(
        (keys_own, sent, up_heads, swa_x, where)
    )
    half = keys_own.shape[0] // 2
    low = from_y(keys_own[:half], 1)
    high = from_y(keys_own[half:], -1)
    keys_other = from_core(keys_own)
    *state, q_all = attend(where[0], (keys_own,), (sent, up_heads), None, False)
    far_own = joined(low, high)
    far_other = from_core(far_own)
    state = attend(where[1], (keys_other,), q_all, state, False)
    partial = attend(where[2], (far_own, far_other), q_all, state, True)
    parts = exchange(partial, "x")
    per_head = out_swa.reshape(x_count, 2, 2 * HEAD, -1)
    from_swa = jnp.zeros((ROWS, out_swa.shape[1]), jnp.float32)
    for values, core in ((swa_x, c_rank), (swa_other, 1 - c_rank)):
        weights = lax.dynamic_index_in_dim(per_head, core, 1, keepdims=False)
        for x in range(x_count):
            from_swa += jnp.dot(values[x], weights[x], preferred_element_type=jnp.float32)
    parts = parts.astype(jnp.float32)
    stats = parts[:, KV_RANK:]
    m = stats[:, 0] + stats[:, 1] + stats[:, 2]
    l = stats[:, 3] + stats[:, 4]
    w = jnp.exp2((m - jnp.max(m, axis=0)) * EXP_SCALE)
    denominator = jnp.sum(l * w, axis=0)
    weighted = jnp.sum(parts[:, :KV_RANK] * w[:, None], axis=0)
    latent_out = (weighted / denominator).astype(jnp.bfloat16)
    up = lax.dynamic_slice_in_dim(value_up, tp_rank * VDIM, VDIM, 1)
    mla_out = lax.dot_general(
        latent_out, up, (((0,), (0,)), ((), ())), preferred_element_type=jnp.float32
    ).astype(jnp.bfloat16)
    all_mla = to_everyone(mla_out, TP)
    from_mla = jnp.einsum(
        "rtd,rdn->tn", all_mla, out_mla.reshape(8, -1, 256), preferred_element_type=jnp.float32
    )
    return (from_mla + from_swa).astype(jnp.bfloat16)


def solution(mesh):
    split = Mesh(mesh.devices.reshape(8, 4, 2, 4, 2), SP_TP)
    placed = (
        P(SP_TP, None),
        P(),
        P(SP, None),
        P(SP, None),
        P(),
        P(None, TP),
        P(),
        P(),
        P(None, TP),
        P(None, TP),
        P(None, TP),
        P(),
        P(None, TP),
        P(None, TP),
    )
    return jax.shard_map(layer, mesh=split, in_specs=placed, out_specs=P(SP, TP), check_vma=False)
```

```python
import functools
import math

import jax
import jax.numpy as jnp
from jax import lax
from jax.experimental import pallas as pl
from jax.experimental.pallas import tpu as pltpu
from jax.sharding import Mesh
from jax.sharding import PartitionSpec as P


NOPE = 128
ROPE = 64
VDIM = 128
KV_RANK = 256
HEAD = 64
WINDOW = 128
SP = ("z", "yh", "yl")
Y = ("yh", "yl")
SAME_PARITY = ("z", "yh")
TP = ("x", "c")
SP_TP = ("z", "yh", "yl", "x", "c")

NORM_EPS = 1e-06
ROPE_BASE = 10000.0
MASKED_VALUE = -1e30
LANES = 128
OWN = 48
SOURCES = 64
ROWS = 384
CHUNK = 16
QTILE = 512
HEADS_CORE = 4
QROWS = HEADS_CORE * ROWS
TILES = QROWS // QTILE
STAT_ROWS = 16
EXP_SCALE = (NOPE + ROPE) ** (-0.5) * math.log2(math.e)


def exchange(array, axis):
    return lax.all_to_all(array, axis, split_axis=0, concat_axis=0, tiled=True)


def to_everyone(array, axis):
    copies = jnp.broadcast_to(array, (lax.axis_size(axis), *array.shape))
    return exchange(copies, axis)


def from_core(value):
    return lax.ppermute(value, "c", [(0, 1), (1, 0)])


def from_x(value, step):
    count = lax.axis_size("x")
    return lax.ppermute(value, "x", [(i, (i + step) % count) for i in range(count)])


def from_y(value, step):
    count = lax.axis_size(Y)
    return lax.ppermute(value, Y, [(i, (i + step) % count) for i in range(count)])


def to_float(values):
    return lax.optimization_barrier(values).astype(jnp.float32)


def norm_rows(values, gains):
    widened = to_float(values)
    scaled = widened * lax.rsqrt(jnp.mean(widened * widened, axis=-1, keepdims=True) + NORM_EPS)
    return (scaled * gains).astype(jnp.bfloat16)


def rotate(values, positions):
    full_width = values.shape[-1]
    half_width = full_width // 2
    inverse = ROPE_BASE ** (-jnp.arange(0, full_width, 2, dtype=jnp.float32) / full_width)
    angles = positions.astype(jnp.float32)[:, None] * inverse[None, :]
    cos_table = jnp.cos(angles)
    sin_table = jnp.sin(angles)
    widened = to_float(values)
    first_half = widened[..., :half_width]
    second_half = widened[..., half_width:]
    return jnp.concatenate(
        [
            first_half * cos_table - second_half * sin_table,
            first_half * sin_table + second_half * cos_table,
        ],
        axis=-1,
    ).astype(jnp.bfloat16)


def attend_body(where_ref, *refs, n_parts, first, last):
    key_refs, refs = refs[:n_parts], refs[n_parts:]
    if first:
        (sent_ref, up_ref, o_ref, m_ref, l_ref, q_ref, kc_ref) = refs
        for h in range(HEADS_CORE):
            rows = pl.ds(h * ROWS, ROWS)
            q_ref[rows, :KV_RANK] = lax.dot_general(
                sent_ref[h, :, :NOPE],
                up_ref[h],
                (((1,), (1,)), ((), ())),
                preferred_element_type=jnp.float32,
            ).astype(jnp.bfloat16)
            q_ref[rows, KV_RANK:] = sent_ref[h, :, NOPE : 2 * LANES]
        o_ref[...] = jnp.zeros_like(o_ref)
        m_ref[...] = jnp.full(m_ref.shape, MASKED_VALUE, jnp.float32)
        l_ref[...] = jnp.zeros_like(l_ref)
    else:
        if last:
            (q_ref, o_in, m_in, l_in, out_ref, o_ref, m_ref, l_ref, kc_ref) = refs
        else:
            (q_ref, o_in, m_in, l_in, o_ref, m_ref, l_ref, kc_ref) = refs
        o_ref[...] = o_in[...]
        m_ref[...] = m_in[...]
        l_ref[...] = l_in[...]
    block = where_ref[0]
    parity = where_ref[1]
    n_keys = CHUNK * OWN

    def load_keys(keys_ref, index):
        part = keys_ref[pl.ds(index * CHUNK, CHUNK)]
        tail = part[:, 2 * OWN :]
        turned = jnp.concatenate([tail[..., ROPE:], tail[..., :ROPE]], axis=-1)
        kc_ref[:, :LANES] = part[:, :OWN].reshape(n_keys, LANES)
        kc_ref[:, LANES : 2 * LANES] = part[:, OWN : 2 * OWN].reshape(n_keys, LANES)
        kc_ref[:, 2 * LANES :] = jnp.concatenate([tail, turned], axis=1).reshape(n_keys, LANES)

    def load_part(part, index):
        if n_parts == 1:
            load_keys(key_refs[0], index)
        for i in range(n_parts if n_parts > 1 else 0):

            @pl.when(part == i)
            def _(i=i):
                load_keys(key_refs[i], index)

    def chunk_step(part, index, masked):
        load_part(part, index)
        if masked:
            row = lax.broadcasted_iota(jnp.int32, (n_keys, 1), 0)
            source = 2 * (index * CHUNK + row // OWN) + parity
            key_pos = source * ROWS + where_ref[2 + part] * OWN + row % OWN

        def scores_of(tile):
            return lax.dot_general(
                kc_ref[...],
                q_ref[tile * QTILE : (tile + 1) * QTILE],
                (((1,), (1,)), ((), ())),
                preferred_element_type=jnp.float32,
            )

        def absorb(tile, s):
            if masked:
                col = tile * QTILE + lax.broadcasted_iota(jnp.int32, (1, QTILE), 1)
                allowed = key_pos <= block * ROWS + col % ROWS
                s = jnp.where(allowed, s, MASKED_VALUE)
            old = m_ref[tile]
            new = jnp.maximum(old, jnp.max(s, axis=0, keepdims=True))
            p = jnp.exp2((s - new) * EXP_SCALE)
            if masked:
                p = jnp.where(allowed, p, 0.0)
            alpha = jnp.exp2((old - new) * EXP_SCALE)
            m_ref[tile] = new
            l_ref[tile] = l_ref[tile] * alpha + jnp.sum(p, axis=0, keepdims=True)
            o_ref[tile] = o_ref[tile] * alpha + lax.dot_general(
                kc_ref[:, : 2 * LANES],
                p.astype(jnp.bfloat16),
                (((0,), (0,)), ((), ())),
                preferred_element_type=jnp.float32,
            )

        s = scores_of(0)
        for tile in range(TILES):
            ahead = scores_of(tile + 1) if tile + 1 < TILES else None
            absorb(tile, s)
            s = ahead

    n_chunks = SOURCES // 2 // CHUNK
    n_full = (block - parity + 1) // (2 * CHUNK)

    def full_step(step, carry):
        if n_parts == 1:
            chunk_step(0, step, False)
        else:
            part = (step >= n_full).astype(jnp.int32)
            chunk_step(part, step - part * n_full, False)
        return carry

    lax.fori_loop(0, n_full * n_parts, full_step, 0)

    @pl.when(n_full < n_chunks)
    def _():
        if n_parts == 1:
            chunk_step(0, n_full, True)
        else:

            def masked_step(part, carry):
                chunk_step(part, n_full, True)
                return carry

            lax.fori_loop(0, n_parts, masked_step, 0)

    if last:
        whole = jnp.concatenate([o_ref[t] for t in range(TILES)], axis=1).astype(jnp.bfloat16)
        m = jnp.concatenate([m_ref[t] for t in range(TILES)], axis=1)
        l = jnp.concatenate([l_ref[t] for t in range(TILES)], axis=1)
        m0 = m.astype(jnp.bfloat16).astype(jnp.float32)
        m1 = (m - m0).astype(jnp.bfloat16).astype(jnp.float32)
        m2 = m - m0 - m1
        l0 = l.astype(jnp.bfloat16).astype(jnp.float32)
        l1 = l - l0
        pad = jnp.zeros((STAT_ROWS - 5, QROWS), jnp.float32)
        stats = jnp.concatenate([m0, m1, m2, l0, l1, pad], axis=0).astype(jnp.bfloat16)
        for h in range(HEADS_CORE):
            out_ref[h, :KV_RANK] = whole[:, h * ROWS : (h + 1) * ROWS]
            out_ref[h, KV_RANK:] = stats[:, h * ROWS : (h + 1) * ROWS]


def attend(where, parts, queries, state, last):
    state_shapes = (
        pltpu.VMEM((TILES, KV_RANK, QTILE), jnp.float32),
        pltpu.VMEM((TILES, 1, QTILE), jnp.float32),
        pltpu.VMEM((TILES, 1, QTILE), jnp.float32),
    )
    first = state is None
    smem = pl.BlockSpec(memory_space=pltpu.SMEM)
    vmem = pl.BlockSpec(memory_space=pltpu.VMEM)
    scratch = [pltpu.VMEM((CHUNK * OWN, 3 * LANES), jnp.bfloat16)]
    out_shape = state_shapes
    if first:
        out_shape = (*state_shapes, pltpu.VMEM((QROWS, 3 * LANES), jnp.bfloat16))
        operands = (where, *parts, *queries)
    else:
        operands = (where, *parts, queries, *state)
    if last:
        out_shape = jax.ShapeDtypeStruct((HEADS_CORE, KV_RANK + STAT_ROWS, ROWS), jnp.bfloat16)
        scratch = list(state_shapes) + scratch
    if not first:
        operands = operands[: 1 + len(parts)] + tuple(
            pltpu.with_memory_space_constraint(value, pltpu.VMEM)
            for value in operands[1 + len(parts) :]
        )
    n_keys = SOURCES // 2 * OWN * len(parts)
    return pl.pallas_call(
        functools.partial(attend_body, n_parts=len(parts), first=first, last=last),
        out_shape=out_shape,
        in_specs=[smem] + [vmem] * (len(operands) - 1),
        out_specs=jax.tree.map(lambda _: vmem, out_shape),
        scratch_shapes=scratch,
        compiler_params=pltpu.CompilerParams(vmem_limit_bytes=24 * 1024 * 1024),
        cost_estimate=pl.CostEstimate(
            flops=2 * QROWS * n_keys * (3 * LANES + KV_RANK),
            transcendentals=QROWS * n_keys,
            bytes_accessed=6000000,
        ),
    )(*operands)


def joined_body(low_ref, high_ref, out_ref):
    half = low_ref.shape[0]
    out_ref[:half] = low_ref[...]
    out_ref[half:] = high_ref[...]


def joined(low, high):
    vmem = pl.BlockSpec(memory_space=pltpu.VMEM)
    return pl.pallas_call(
        joined_body,
        out_shape=jax.ShapeDtypeStruct((2 * low.shape[0], *low.shape[1:]), low.dtype),
        in_specs=[vmem, vmem],
        out_specs=vmem,
        compiler_params=pltpu.CompilerParams(vmem_limit_bytes=8 * 1024 * 1024),
        name="joined",
    )(low, high)


def windowed_body(where_ref, sink_ref, q_ref, kv_ref, before_ref, query_ref, out_ref):
    out_ref[:, : 2 * LANES] = query_ref[...]
    for tile in range(ROWS // WINDOW):
        q = q_ref[tile * WINDOW : (tile + 1) * WINDOW]
        here = kv_ref[tile * WINDOW : (tile + 1) * WINDOW]
        if tile == 0:
            behind = before_ref[...]
        else:
            behind = kv_ref[(tile - 1) * WINDOW : tile * WINDOW]
        both = jnp.concatenate([behind, here], axis=0)
        row = lax.broadcasted_iota(jnp.int32, (WINDOW, 2 * WINDOW), 0)
        col = lax.broadcasted_iota(jnp.int32, (WINDOW, 2 * WINDOW), 1)
        allowed = (col > row) & (col <= row + WINDOW)
        if tile == 0:
            allowed = allowed & ((col >= WINDOW) | (where_ref[0] > 0))
        outs = []
        for h in range(LANES // HEAD):
            scores = lax.dot_general(
                q[:, h * HEAD : (h + 1) * HEAD],
                both[:, :HEAD],
                (((1,), (1,)), ((), ())),
                preferred_element_type=jnp.float32,
            ) * HEAD ** (-0.5)
            scores = jnp.where(allowed, scores, MASKED_VALUE)
            sink = jnp.full((WINDOW, 1), sink_ref[where_ref[2] * (LANES // HEAD) + h])
            row_max = jnp.maximum(jnp.max(scores, axis=1, keepdims=True), sink)
            raw = jnp.exp(scores - row_max)
            total = jnp.sum(raw, axis=1, keepdims=True) + jnp.exp(sink - row_max)
            weights = (raw / total).astype(jnp.bfloat16)
            outs.append(jnp.dot(weights, both[:, HEAD:], preferred_element_type=jnp.float32))
        out_ref[tile * WINDOW : (tile + 1) * WINDOW, 2 * LANES :] = jnp.concatenate(
            outs, axis=1
        ).astype(jnp.bfloat16)


def windowed(where, sink_logits, q, kv, before, query):
    smem = pl.BlockSpec(memory_space=pltpu.SMEM)
    vmem = pl.BlockSpec(memory_space=pltpu.VMEM)
    return pl.pallas_call(
        windowed_body,
        out_shape=jax.ShapeDtypeStruct((ROWS, 3 * LANES), jnp.bfloat16),
        in_specs=[smem, smem, vmem, vmem, vmem, vmem],
        out_specs=vmem,
        compiler_params=pltpu.CompilerParams(vmem_limit_bytes=16 * 1024 * 1024),
        cost_estimate=pl.CostEstimate(
            flops=4 * ROWS * 2 * WINDOW * LANES,
            transcendentals=ROWS * 4 * WINDOW,
            bytes_accessed=1000000,
        ),
        name="windowed",
    )(where, sink_logits, q, kv, before, query)


def layer(
    inputs,
    norm_gain,
    latent_down,
    rope_down,
    latent_gain,
    mla_query,
    key_up,
    value_up,
    swa_query,
    swa_key,
    swa_value,
    sink_logits,
    out_mla,
    out_swa,
):
    own_rows = inputs.shape[0]
    x_rank = lax.axis_index("x")
    c_rank = lax.axis_index("c")
    tp_rank = lax.axis_index(TP)
    block = lax.axis_index(SP)
    offset = block * ROWS
    own_pos = offset + tp_rank * own_rows + jnp.arange(own_rows, dtype=jnp.int32)
    block_pos = offset + jnp.arange(ROWS, dtype=jnp.int32)

    x_count = lax.axis_size("x")

    def by_x(values):
        placed = jnp.zeros((x_count, *values.shape), values.dtype)
        arrived = [values] + [from_x(values, k) for k in range(1, x_count)]
        for k, value in enumerate(arrived):
            at = (x_rank - k) % x_count
            placed = lax.dynamic_update_index_in_dim(placed, value, at, 0)
        return placed

    def by_core(values):
        return tuple(
            lax.dynamic_index_in_dim(values, rank, 0, keepdims=False)
            for rank in (c_rank, 1 - c_rank)
        )

    def by_core(values):
        return tuple(
            lax.dynamic_index_in_dim(values, rank, 0, keepdims=False)
            for rank in (c_rank, 1 - c_rank)
        )

    down = jnp.concatenate([latent_down, rope_down], axis=1)
    width = down.shape[1] // x_count
    down = lax.dynamic_slice_in_dim(down, x_rank * width, width, 1)
    rest = LANES - width
    low, high = (down[:16], down[16:])
    bottom = jnp.concatenate([high[:8, rest:], high[8:, rest:]], axis=1)
    bottom = jnp.pad(bottom, ((0, 0), (0, LANES - bottom.shape[1])))
    down = jnp.concatenate([jnp.concatenate([low, high[:, :rest]], axis=1), bottom], axis=0)
    down = to_everyone(down, SP)
    left = width - rest
    ends = jnp.concatenate([down[:, 16:, :left], down[:, 16:, left : 2 * left]], axis=1)
    high = jnp.concatenate([down[:, :16, width:], ends], axis=2)
    down = jnp.stack([down[:, :16, :width], high], axis=1).reshape(-1, width)

    normed = norm_rows(inputs, norm_gain)
    kv_weights = jnp.concatenate([swa_key, swa_value], axis=1)
    mine = by_x(normed)
    mine = lax.optimization_barrier(mine)
    kv_weights_other = from_core(kv_weights)

    latent = jnp.dot(mine.reshape(-1, mine.shape[2]), down, preferred_element_type=jnp.float32)
    latent = latent.astype(jnp.bfloat16).reshape(x_count, own_rows, width)
    latent = exchange(latent, "x")
    tail_rows = mine[x_count // 2 :].reshape(2 * own_rows, -1)
    tail = jnp.concatenate(
        [
            jnp.dot(tail_rows, weights, preferred_element_type=jnp.float32)
            for weights in (kv_weights, kv_weights_other)
        ],
        axis=1,
    ).astype(jnp.bfloat16)
    count = lax.axis_size(SP)
    before = lax.ppermute(tail, SP, [(i, i + 1) for i in range(count - 1)])
    latent = jnp.transpose(latent, (1, 0, 2)).reshape(own_rows, KV_RANK + ROPE)
    keys_latent = norm_rows(latent[:, :KV_RANK], latent_gain)
    keys_rope = rotate(latent[:, KV_RANK:], own_pos)
    packed = jnp.concatenate(
        [
            keys_latent[:, :LANES],
            keys_latent[:, LANES:],
            jnp.concatenate([keys_rope[: OWN // 2], keys_rope[OWN // 2 :]], axis=1),
        ],
        axis=0,
    )
    up_heads = jnp.stack(
        [lax.dynamic_slice_in_dim(key_up, (2 * x + c_rank) * NOPE, NOPE, 1) for x in range(x_count)]
    )
    parity = lax.axis_index("yl")
    rank_other = tp_rank + 1 - 2 * c_rank
    where = [
        jnp.stack(entries).astype(jnp.int32)
        for entries in (
            (block, parity, tp_rank),
            (block, parity, rank_other),
            (block, 1 - parity, tp_rank, rank_other),
        )
    ]
    packed, mine, before, where = lax.optimization_barrier((packed, mine, before, where))
    keys_own = to_everyone(packed, SAME_PARITY)

    other = from_core(mine)
    pieces = jnp.zeros((x_count, 2, *mine.shape[1:]), jnp.bfloat16)
    pieces = lax.dynamic_update_index_in_dim(pieces, mine, c_rank, 1)
    pieces = lax.dynamic_update_index_in_dim(pieces, other, 1 - c_rank, 1)
    pieces = pieces.reshape(ROWS, -1)
    before_other = from_core(before[:, LANES:])
    before_both = jnp.stack([before[:, :LANES], before_other])
    rows_0, rows_1 = by_core(before_both)
    before = jnp.concatenate([rows_1[3 * OWN - WINDOW : OWN], rows_0[OWN:], rows_1[OWN:]], axis=0)
    swa_kv = jnp.dot(pieces, kv_weights, preferred_element_type=jnp.float32)
    swa_kv = swa_kv.astype(jnp.bfloat16)
    swa_q = jnp.dot(pieces, swa_query, preferred_element_type=jnp.float32)
    swa_q = swa_q.astype(jnp.bfloat16)
    queries = jnp.dot(pieces, mla_query, preferred_element_type=jnp.float32)
    queries = queries.astype(jnp.bfloat16)
    query = jnp.concatenate(
        [
            queries[:, :NOPE],
            rotate(queries[:, NOPE:], block_pos),
            jnp.zeros((ROWS, LANES - ROPE), jnp.bfloat16),
        ],
        axis=1,
    )
    sent = windowed(where[0], sink_logits, swa_q, swa_kv, before, query)
    sent = by_x(sent)
    keys_own, sent, up_heads, where = lax.optimization_barrier((keys_own, sent, up_heads, where))
    half = keys_own.shape[0] // 2
    low = from_y(keys_own[:half], 1)
    high = from_y(keys_own[half:], -1)
    keys_other = from_core(keys_own)
    *state, q_all = attend(where[0], (keys_own,), (sent, up_heads), None, False)
    far_own = joined(low, high)
    far_other = from_core(far_own)
    state = attend(where[1], (keys_other,), q_all, state, False)
    partial = attend(where[2], (far_own, far_other), q_all, state, True)
    parts = exchange(partial, "x")
    swa_x = lax.optimization_barrier(sent[:, :, 2 * LANES :])
    swa_other = from_core(swa_x)
    per_head = out_swa.reshape(x_count, 2, 2 * HEAD, -1)
    from_swa = jnp.zeros((ROWS, out_swa.shape[1]), jnp.float32)
    for values, core in ((swa_x, c_rank), (swa_other, 1 - c_rank)):
        weights = lax.dynamic_index_in_dim(per_head, core, 1, keepdims=False)
        for x in range(x_count):
            from_swa += jnp.dot(values[x], weights[x], preferred_element_type=jnp.float32)
    parts = parts.astype(jnp.float32)
    stats = parts[:, KV_RANK:]
    m = stats[:, 0] + stats[:, 1] + stats[:, 2]
    l = stats[:, 3] + stats[:, 4]
    w = jnp.exp2((m - jnp.max(m, axis=0)) * EXP_SCALE)
    denominator = jnp.sum(l * w, axis=0)
    weighted = jnp.sum(parts[:, :KV_RANK] * w[:, None], axis=0)
    latent_out = (weighted / denominator).astype(jnp.bfloat16)
    up = lax.dynamic_slice_in_dim(value_up, tp_rank * VDIM, VDIM, 1)
    mla_out = lax.dot_general(
        latent_out, up, (((0,), (0,)), ((), ())), preferred_element_type=jnp.float32
    ).astype(jnp.bfloat16)
    all_mla = to_everyone(mla_out, TP)
    from_mla = jnp.einsum(
        "rtd,rdn->tn", all_mla, out_mla.reshape(8, -1, 256), preferred_element_type=jnp.float32
    )
    return (from_mla + from_swa).astype(jnp.bfloat16)


def solution(mesh):
    split = Mesh(mesh.devices.reshape(8, 4, 2, 4, 2), SP_TP)
    placed = (
        P(SP_TP, None),
        P(),
        P(SP, None),
        P(SP, None),
        P(),
        P(None, TP),
        P(),
        P(),
        P(None, TP),
        P(None, TP),
        P(None, TP),
        P(),
        P(None, TP),
        P(None, TP),
    )
    return jax.shard_map(layer, mesh=split, in_specs=placed, out_specs=P(SP, TP), check_vma=False)
```

```python
import functools
import math

import jax
import jax.numpy as jnp
from jax import lax
from jax.experimental import pallas as pl
from jax.experimental.pallas import tpu as pltpu
from jax.sharding import Mesh
from jax.sharding import PartitionSpec as P


NOPE = 128
ROPE = 64
VDIM = 128
KV_RANK = 256
HEAD = 64
WINDOW = 128
SP = ("z", "yh", "yl")
Y = ("yh", "yl")
SAME_PARITY = ("z", "yh")
TP = ("x", "c")
SP_TP = ("z", "yh", "yl", "x", "c")

NORM_EPS = 1e-06
ROPE_BASE = 10000.0
MASKED_VALUE = -1e30
LANES = 128
OWN = 48
SOURCES = 64
ROWS = 384
CHUNK = 16
QTILE = 512
HEADS_CORE = 4
QROWS = HEADS_CORE * ROWS
TILES = QROWS // QTILE
STAT_ROWS = 16
EXP_SCALE = (NOPE + ROPE) ** (-0.5) * math.log2(math.e)


def exchange(array, axis):
    return lax.all_to_all(array, axis, split_axis=0, concat_axis=0, tiled=True)


def to_everyone(array, axis):
    copies = jnp.broadcast_to(array, (lax.axis_size(axis), *array.shape))
    return exchange(copies, axis)


def from_core(value):
    return lax.ppermute(value, "c", [(0, 1), (1, 0)])


def from_x(value, step):
    count = lax.axis_size("x")
    return lax.ppermute(value, "x", [(i, (i + step) % count) for i in range(count)])


def from_y(value, step):
    count = lax.axis_size(Y)
    return lax.ppermute(value, Y, [(i, (i + step) % count) for i in range(count)])


def to_float(values):
    return lax.optimization_barrier(values).astype(jnp.float32)


def norm_rows(values, gains):
    widened = to_float(values)
    scaled = widened * lax.rsqrt(jnp.mean(widened * widened, axis=-1, keepdims=True) + NORM_EPS)
    return (scaled * gains).astype(jnp.bfloat16)


def rotate(values, positions):
    full_width = values.shape[-1]
    half_width = full_width // 2
    inverse = ROPE_BASE ** (-jnp.arange(0, full_width, 2, dtype=jnp.float32) / full_width)
    angles = positions.astype(jnp.float32)[:, None] * inverse[None, :]
    cos_table = jnp.cos(angles)
    sin_table = jnp.sin(angles)
    widened = to_float(values)
    first_half = widened[..., :half_width]
    second_half = widened[..., half_width:]
    return jnp.concatenate(
        [
            first_half * cos_table - second_half * sin_table,
            first_half * sin_table + second_half * cos_table,
        ],
        axis=-1,
    ).astype(jnp.bfloat16)


def attend_body(where_ref, *refs, n_parts, first, last):
    key_refs, refs = refs[:n_parts], refs[n_parts:]
    if first:
        (sent_ref, up_ref, o_ref, m_ref, l_ref, q_ref, kc_ref) = refs
        for h in range(HEADS_CORE):
            rows = pl.ds(h * ROWS, ROWS)
            q_ref[rows, :KV_RANK] = lax.dot_general(
                sent_ref[h, :, :NOPE],
                up_ref[h],
                (((1,), (1,)), ((), ())),
                preferred_element_type=jnp.float32,
            ).astype(jnp.bfloat16)
            q_ref[rows, KV_RANK:] = sent_ref[h, :, NOPE : 2 * LANES]
        o_ref[...] = jnp.zeros_like(o_ref)
        m_ref[...] = jnp.full(m_ref.shape, MASKED_VALUE, jnp.float32)
        l_ref[...] = jnp.zeros_like(l_ref)
    else:
        if last:
            (q_ref, o_in, m_in, l_in, out_ref, o_ref, m_ref, l_ref, kc_ref) = refs
        else:
            (q_ref, o_in, m_in, l_in, o_ref, m_ref, l_ref, kc_ref) = refs
        o_ref[...] = o_in[...]
        m_ref[...] = m_in[...]
        l_ref[...] = l_in[...]
    block = where_ref[0]
    parity = where_ref[1]
    n_keys = CHUNK * OWN

    def load_keys(keys_ref, index):
        part = keys_ref[pl.ds(index * CHUNK, CHUNK)]
        tail = part[:, 2 * OWN :]
        turned = jnp.concatenate([tail[..., ROPE:], tail[..., :ROPE]], axis=-1)
        kc_ref[:, :LANES] = part[:, :OWN].reshape(n_keys, LANES)
        kc_ref[:, LANES : 2 * LANES] = part[:, OWN : 2 * OWN].reshape(n_keys, LANES)
        kc_ref[:, 2 * LANES :] = jnp.concatenate([tail, turned], axis=1).reshape(n_keys, LANES)

    def load_part(part, index):
        if n_parts == 1:
            load_keys(key_refs[0], index)
        for i in range(n_parts if n_parts > 1 else 0):

            @pl.when(part == i)
            def _(i=i):
                load_keys(key_refs[i], index)

    def chunk_step(part, index, masked):
        load_part(part, index)
        if masked:
            row = lax.broadcasted_iota(jnp.int32, (n_keys, 1), 0)
            source = 2 * (index * CHUNK + row // OWN) + parity
            key_pos = source * ROWS + where_ref[2 + part] * OWN + row % OWN

        def scores_of(tile):
            return lax.dot_general(
                kc_ref[...],
                q_ref[tile * QTILE : (tile + 1) * QTILE],
                (((1,), (1,)), ((), ())),
                preferred_element_type=jnp.float32,
            )

        def absorb(tile, s):
            if masked:
                col = tile * QTILE + lax.broadcasted_iota(jnp.int32, (1, QTILE), 1)
                allowed = key_pos <= block * ROWS + col % ROWS
                s = jnp.where(allowed, s, MASKED_VALUE)
            old = m_ref[tile]
            new = jnp.maximum(old, jnp.max(s, axis=0, keepdims=True))
            p = jnp.exp2((s - new) * EXP_SCALE)
            if masked:
                p = jnp.where(allowed, p, 0.0)
            alpha = jnp.exp2((old - new) * EXP_SCALE)
            m_ref[tile] = new
            l_ref[tile] = l_ref[tile] * alpha + jnp.sum(p, axis=0, keepdims=True)
            o_ref[tile] = o_ref[tile] * alpha + lax.dot_general(
                kc_ref[:, : 2 * LANES],
                p.astype(jnp.bfloat16),
                (((0,), (0,)), ((), ())),
                preferred_element_type=jnp.float32,
            )

        s = scores_of(0)
        for tile in range(TILES):
            ahead = scores_of(tile + 1) if tile + 1 < TILES else None
            absorb(tile, s)
            s = ahead

    n_chunks = SOURCES // 2 // CHUNK
    n_full = (block - parity + 1) // (2 * CHUNK)

    def full_step(step, carry):
        if n_parts == 1:
            chunk_step(0, step, False)
        else:
            part = (step >= n_full).astype(jnp.int32)
            chunk_step(part, step - part * n_full, False)
        return carry

    lax.fori_loop(0, n_full * n_parts, full_step, 0)

    @pl.when(n_full < n_chunks)
    def _():
        if n_parts == 1:
            chunk_step(0, n_full, True)
        else:

            def masked_step(part, carry):
                chunk_step(part, n_full, True)
                return carry

            lax.fori_loop(0, n_parts, masked_step, 0)

    if last:
        whole = jnp.concatenate([o_ref[t] for t in range(TILES)], axis=1).astype(jnp.bfloat16)
        m = jnp.concatenate([m_ref[t] for t in range(TILES)], axis=1)
        l = jnp.concatenate([l_ref[t] for t in range(TILES)], axis=1)
        m0 = m.astype(jnp.bfloat16).astype(jnp.float32)
        m1 = (m - m0).astype(jnp.bfloat16).astype(jnp.float32)
        m2 = m - m0 - m1
        l0 = l.astype(jnp.bfloat16).astype(jnp.float32)
        l1 = l - l0
        pad = jnp.zeros((STAT_ROWS - 5, QROWS), jnp.float32)
        stats = jnp.concatenate([m0, m1, m2, l0, l1, pad], axis=0).astype(jnp.bfloat16)
        for h in range(HEADS_CORE):
            out_ref[h, :KV_RANK] = whole[:, h * ROWS : (h + 1) * ROWS]
            out_ref[h, KV_RANK:] = stats[:, h * ROWS : (h + 1) * ROWS]


def attend(where, parts, queries, state, last):
    state_shapes = (
        pltpu.VMEM((TILES, KV_RANK, QTILE), jnp.float32),
        pltpu.VMEM((TILES, 1, QTILE), jnp.float32),
        pltpu.VMEM((TILES, 1, QTILE), jnp.float32),
    )
    first = state is None
    smem = pl.BlockSpec(memory_space=pltpu.SMEM)
    vmem = pl.BlockSpec(memory_space=pltpu.VMEM)
    scratch = [pltpu.VMEM((CHUNK * OWN, 3 * LANES), jnp.bfloat16)]
    out_shape = state_shapes
    if first:
        out_shape = (*state_shapes, pltpu.VMEM((QROWS, 3 * LANES), jnp.bfloat16))
        operands = (where, *parts, *queries)
    else:
        operands = (where, *parts, queries, *state)
    if last:
        out_shape = jax.ShapeDtypeStruct((HEADS_CORE, KV_RANK + STAT_ROWS, ROWS), jnp.bfloat16)
        scratch = list(state_shapes) + scratch
    if not first:
        operands = operands[: 1 + len(parts)] + tuple(
            pltpu.with_memory_space_constraint(value, pltpu.VMEM)
            for value in operands[1 + len(parts) :]
        )
    n_keys = SOURCES // 2 * OWN * len(parts)
    return pl.pallas_call(
        functools.partial(attend_body, n_parts=len(parts), first=first, last=last),
        out_shape=out_shape,
        in_specs=[smem] + [vmem] * (len(operands) - 1),
        out_specs=jax.tree.map(lambda _: vmem, out_shape),
        scratch_shapes=scratch,
        compiler_params=pltpu.CompilerParams(vmem_limit_bytes=24 * 1024 * 1024),
        cost_estimate=pl.CostEstimate(
            flops=2 * QROWS * n_keys * (3 * LANES + KV_RANK),
            transcendentals=QROWS * n_keys,
            bytes_accessed=6000000,
        ),
    )(*operands)


def joined_body(low_ref, high_ref, out_ref):
    half = low_ref.shape[0]
    out_ref[:half] = low_ref[...]
    out_ref[half:] = high_ref[...]


def joined(low, high):
    vmem = pl.BlockSpec(memory_space=pltpu.VMEM)
    return pl.pallas_call(
        joined_body,
        out_shape=jax.ShapeDtypeStruct((2 * low.shape[0], *low.shape[1:]), low.dtype),
        in_specs=[vmem, vmem],
        out_specs=vmem,
        compiler_params=pltpu.CompilerParams(vmem_limit_bytes=8 * 1024 * 1024),
        name="joined",
    )(low, high)


def windowed_body(where_ref, sink_ref, rows_ref, before_ref, query_ref, out_ref):
    out_ref[:, : 2 * LANES] = query_ref[...]
    for tile in range(ROWS // WINDOW):
        here = rows_ref[tile * WINDOW : (tile + 1) * WINDOW]
        if tile == 0:
            behind = before_ref[...]
        else:
            behind = rows_ref[(tile - 1) * WINDOW : tile * WINDOW, LANES:]
        both = jnp.concatenate([behind, here[:, LANES:]], axis=0)
        row = lax.broadcasted_iota(jnp.int32, (WINDOW, 2 * WINDOW), 0)
        col = lax.broadcasted_iota(jnp.int32, (WINDOW, 2 * WINDOW), 1)
        allowed = (col > row) & (col <= row + WINDOW)
        if tile == 0:
            allowed = allowed & ((col >= WINDOW) | (where_ref[0] > 0))
        outs = []
        for h in range(LANES // HEAD):
            scores = lax.dot_general(
                here[:, h * HEAD : (h + 1) * HEAD],
                both[:, :HEAD],
                (((1,), (1,)), ((), ())),
                preferred_element_type=jnp.float32,
            ) * HEAD ** (-0.5)
            scores = jnp.where(allowed, scores, MASKED_VALUE)
            sink = jnp.full((WINDOW, 1), sink_ref[where_ref[2] * (LANES // HEAD) + h])
            row_max = jnp.maximum(jnp.max(scores, axis=1, keepdims=True), sink)
            raw = jnp.exp(scores - row_max)
            total = jnp.sum(raw, axis=1, keepdims=True) + jnp.exp(sink - row_max)
            weights = (raw / total).astype(jnp.bfloat16)
            outs.append(jnp.dot(weights, both[:, HEAD:], preferred_element_type=jnp.float32))
        out_ref[tile * WINDOW : (tile + 1) * WINDOW, 2 * LANES :] = jnp.concatenate(
            outs, axis=1
        ).astype(jnp.bfloat16)


def windowed(where, sink_logits, rows, before, query):
    smem = pl.BlockSpec(memory_space=pltpu.SMEM)
    vmem = pl.BlockSpec(memory_space=pltpu.VMEM)
    return pl.pallas_call(
        windowed_body,
        out_shape=jax.ShapeDtypeStruct((ROWS, 3 * LANES), jnp.bfloat16),
        in_specs=[smem, smem, vmem, vmem, vmem],
        out_specs=vmem,
        compiler_params=pltpu.CompilerParams(vmem_limit_bytes=16 * 1024 * 1024),
        cost_estimate=pl.CostEstimate(
            flops=4 * ROWS * 2 * WINDOW * LANES,
            transcendentals=ROWS * 4 * WINDOW,
            bytes_accessed=1000000,
        ),
        name="windowed",
    )(where, sink_logits, rows, before, query)


def layer(
    inputs,
    norm_gain,
    latent_down,
    rope_down,
    latent_gain,
    mla_query,
    key_up,
    value_up,
    swa_query,
    swa_key,
    swa_value,
    sink_logits,
    out_mla,
    out_swa,
):
    own_rows = inputs.shape[0]
    x_rank = lax.axis_index("x")
    c_rank = lax.axis_index("c")
    tp_rank = lax.axis_index(TP)
    block = lax.axis_index(SP)
    offset = block * ROWS
    own_pos = offset + tp_rank * own_rows + jnp.arange(own_rows, dtype=jnp.int32)
    block_pos = offset + jnp.arange(ROWS, dtype=jnp.int32)

    x_count = lax.axis_size("x")

    def by_x(values):
        placed = jnp.zeros((x_count, *values.shape), values.dtype)
        arrived = [values] + [from_x(values, k) for k in range(1, x_count)]
        for k, value in enumerate(arrived):
            at = (x_rank - k) % x_count
            placed = lax.dynamic_update_index_in_dim(placed, value, at, 0)
        return placed

    half = rope_down.shape[0] // 2
    down = jnp.concatenate(
        [
            latent_down[:, :LANES],
            latent_down[:, LANES:],
            jnp.concatenate([rope_down[:half], rope_down[half:]], axis=1),
        ],
        axis=0,
    )
    down = to_everyone(down, SP)
    rope_tiles = down[:, 4 * half :]
    down_rope = jnp.stack([rope_tiles[:, :, :ROPE], rope_tiles[:, :, ROPE:]], axis=1)
    down_rope = down_rope.reshape(-1, ROPE)
    down_latent = jnp.concatenate([down[:, : 2 * half], down[:, 2 * half : 4 * half]], axis=2)
    down_latent = down_latent.reshape(-1, KV_RANK)

    normed = norm_rows(inputs, norm_gain)
    swa_weights = jnp.concatenate([swa_query, swa_key, swa_value], axis=1)
    mine = by_x(normed)
    other = from_core(mine)
    pieces = jnp.zeros((x_count, 2, *mine.shape[1:]), jnp.bfloat16)
    pieces = lax.dynamic_update_index_in_dim(pieces, mine, c_rank, 1)
    pieces = lax.dynamic_update_index_in_dim(pieces, other, 1 - c_rank, 1)
    pieces = pieces.reshape(ROWS, -1)
    swa_rows = jnp.dot(pieces, swa_weights, preferred_element_type=jnp.float32)
    swa_rows = swa_rows.astype(jnp.bfloat16)
    count = lax.axis_size(SP)
    before = lax.ppermute(
        swa_rows[ROWS - WINDOW :, LANES:], SP, [(i, i + 1) for i in range(count - 1)]
    )
    queries = jnp.dot(pieces, mla_query, preferred_element_type=jnp.float32)
    queries = queries.astype(jnp.bfloat16)
    query = jnp.concatenate(
        [
            queries[:, :NOPE],
            rotate(queries[:, NOPE:], block_pos),
            jnp.zeros((ROWS, LANES - ROPE), jnp.bfloat16),
        ],
        axis=1,
    )

    latent = jnp.dot(normed, down_latent, preferred_element_type=jnp.float32)
    rope_raw = jnp.dot(normed, down_rope, preferred_element_type=jnp.float32)
    keys_latent = norm_rows(latent.astype(jnp.bfloat16), latent_gain)
    keys_rope = rotate(rope_raw.astype(jnp.bfloat16), own_pos)
    packed = jnp.concatenate(
        [
            keys_latent[:, :LANES],
            keys_latent[:, LANES:],
            jnp.concatenate([keys_rope[: OWN // 2], keys_rope[OWN // 2 :]], axis=1),
        ],
        axis=0,
    )
    up_heads = jnp.stack(
        [lax.dynamic_slice_in_dim(key_up, (2 * x + c_rank) * NOPE, NOPE, 1) for x in range(x_count)]
    )
    parity = lax.axis_index("yl")
    rank_other = tp_rank + 1 - 2 * c_rank
    where = [
        jnp.stack(entries).astype(jnp.int32)
        for entries in (
            (block, parity, tp_rank),
            (block, parity, rank_other),
            (block, 1 - parity, tp_rank, rank_other),
        )
    ]
    packed, swa_rows, before, query, up_heads, where = lax.optimization_barrier(
        (packed, swa_rows, before, query, up_heads, where)
    )
    keys_own = to_everyone(packed, SAME_PARITY)

    sent = windowed(where[0], sink_logits, swa_rows, before, query)
    sent = by_x(sent)
    keys_own, sent, up_heads, where = lax.optimization_barrier((keys_own, sent, up_heads, where))
    half = keys_own.shape[0] // 2
    low = from_y(keys_own[:half], 1)
    high = from_y(keys_own[half:], -1)
    keys_other = from_core(keys_own)
    *state, q_all = attend(where[0], (keys_own,), (sent, up_heads), None, False)
    far_own = joined(low, high)
    far_other = from_core(far_own)
    state = attend(where[1], (keys_other,), q_all, state, False)
    partial = attend(where[2], (far_own, far_other), q_all, state, True)
    parts = exchange(partial, "x")
    swa_x = lax.optimization_barrier(sent[:, :, 2 * LANES :])
    swa_other = from_core(swa_x)
    per_head = out_swa.reshape(x_count, 2, 2 * HEAD, -1)
    from_swa = jnp.zeros((ROWS, out_swa.shape[1]), jnp.float32)
    for values, core in ((swa_x, c_rank), (swa_other, 1 - c_rank)):
        weights = lax.dynamic_index_in_dim(per_head, core, 1, keepdims=False)
        for x in range(x_count):
            from_swa += jnp.dot(values[x], weights[x], preferred_element_type=jnp.float32)
    parts = parts.astype(jnp.float32)
    stats = parts[:, KV_RANK:]
    m = stats[:, 0] + stats[:, 1] + stats[:, 2]
    l = stats[:, 3] + stats[:, 4]
    w = jnp.exp2((m - jnp.max(m, axis=0)) * EXP_SCALE)
    denominator = jnp.sum(l * w, axis=0)
    weighted = jnp.sum(parts[:, :KV_RANK] * w[:, None], axis=0)
    latent_out = (weighted / denominator).astype(jnp.bfloat16)
    up = lax.dynamic_slice_in_dim(value_up, tp_rank * VDIM, VDIM, 1)
    mla_out = lax.dot_general(
        latent_out, up, (((0,), (0,)), ((), ())), preferred_element_type=jnp.float32
    ).astype(jnp.bfloat16)
    all_mla = to_everyone(mla_out, TP)
    from_mla = jnp.einsum(
        "rtd,rdn->tn", all_mla, out_mla.reshape(8, -1, 256), preferred_element_type=jnp.float32
    )
    return (from_mla + from_swa).astype(jnp.bfloat16)


def solution(mesh):
    split = Mesh(mesh.devices.reshape(8, 4, 2, 4, 2), SP_TP)
    placed = (
        P(SP_TP, None),
        P(),
        P(SP, None),
        P(SP, None),
        P(),
        P(None, TP),
        P(),
        P(),
        P(None, TP),
        P(None, TP),
        P(None, TP),
        P(),
        P(None, TP),
        P(None, TP),
    )
    return jax.shard_map(layer, mesh=split, in_specs=placed, out_specs=P(SP, TP), check_vma=False)
```
